32 devices in a mesh: ep: 4 (over y, x), tp: 8 (over z, core).
Axes of the slice: x: 2, y: 2, z: 4, core: 2. Of those that a mesh axis runs over, the one named last changes fastest.
Arguments:
- tokens: bfloat16 [128, 2048], P(('ep', 'tp')), may hold values from -6 to 6
- lengths: int32 [128], P(('ep', 'tp')), may hold values from 64 to 1024
- cache_latent: bfloat16 [128, 1024, 512], P(('ep', 'tp')), may hold values from -6 to 6
- cache_rope_key: bfloat16 [128, 1024, 32], P(('ep', 'tp')), may hold values from -1000 to 1000
- route_ids: int32 [128, 4], P('ep'), may hold values from 0 to 31, all different within a row; in each aligned block of 32 rows (0 to 31, 32 to 63, ...) at most 8 rows name the same one
- route_weights: float32 [128, 4], P('ep'), may hold values from 0.2 to 2
- attn_gain: float32 [2048], replicated, may hold values from 0.1 to 1.9
- w_query_nope: bfloat16 [2048, 16, 64], P(None, 'tp'), may hold values from -0.125 to 0.125
- w_query_rope: bfloat16 [2048, 16, 32], P(None, 'tp'), may hold values from -0.125 to 0.125
- w_latent_down: bfloat16 [2048, 512], P(None, 'tp'), may hold values from -0.125 to 0.125
- w_key_rope: bfloat16 [2048, 32], replicated, may hold values from -0.125 to 0.125
- latent_gain: float32 [512], replicated, may hold values from 0.1 to 1.9
- w_key_up: bfloat16 [512, 16, 64], P(None, 'tp'), may hold values from -0.75 to 0.75
- w_value_up: bfloat16 [512, 16, 64], P(None, 'tp'), may hold values from -0.25 to 0.25
- w_attn_out: bfloat16 [16, 64, 2048], P('tp'), may hold values from -0.1875 to 0.1875
- ffn_gain: float32 [2048], replicated, may hold values from 0.1 to 1.9
- expert_gate: bfloat16 [32, 2048, 512], P(('ep', 'tp')), may hold values from -0.125 to 0.125
- expert_up: bfloat16 [32, 2048, 512], P(('ep', 'tp')), may hold values from -0.125 to 0.125
- expert_down: bfloat16 [32, 512, 2048], P(('ep', 'tp')), may hold values from -0.25 to 0.25
- shared_gate: bfloat16 [2048, 512], P(None, 'tp'), may hold values from -0.125 to 0.125
- shared_up: bfloat16 [2048, 512], P(None, 'tp'), may hold values from -0.125 to 0.125
- shared_down: bfloat16 [512, 2048], P('tp'), may hold values from -0.25 to 0.25
- dense_gate: bfloat16 [2048, 1024], P(None, 'tp'), may hold values from -0.125 to 0.125
- dense_up: bfloat16 [2048, 1024], P(None, 'tp'), may hold values from -0.125 to 0.125
- dense_down: bfloat16 [1024, 2048], P('tp'), may hold values from -0.1875 to 0.1875
- branch_gate: bfloat16 [2048], replicated, may hold values from -0.125 to 0.125
Outputs:
- mixed: bfloat16 [128, 2048], P(('ep', 'tp'))
- new_latent: bfloat16 [128, 512], P(('ep', 'tp'))
- new_rope_key: bfloat16 [128, 32], P(('ep', 'tp'))
The draws below stay inside these ranges and needn't reach their ends.
Inputs may be any that keep to these rules, and one draw needn't show every extreme that they name: `route_ids`: in each aligned block of 32 rows, no expert is named by more than 8 of the block's rows, a bound that some block reaches. Each row names 4 different experts.
All inputs are finite; a program needn't handle non-finite values.
Results may differ from the reference program's by a relative error of at most 0.025.
Values may be sent and summed in bfloat16 or wider, within the bound.
A program may use at most 64 MiB of HBM per device.

```python
import math
import jax
import jax.numpy as jnp
import numpy as np
from jax import lax

D = 2048
HEADS = 16
NOPE = 64
ROPE = 32
VHEAD = 64
LATENT = 512
EXPERT_FF = 512
SHARED_FF = 512
DENSE_FF = 1024
TOP_K = 4
LEN = 1024
GROUP = 32
SEQS = 128
EXPERTS = 32
CAP = 8
N_EP = 4


def draw_cache_rope_key(key, part):
    values = jnp.clip(jax.random.normal(key, (SEQS, LEN, ROPE), jnp.float32), -6.0, 6.0)
    return values.astype(jnp.bfloat16)


def plant(array, rng, low, top_value):
    longest = array.shape.index(max(array.shape))
    spots = []
    for shift in (0, 1):
        where = [jax.random.randint(jax.random.fold_in(rng, axis), (), 0, length) for axis, length in enumerate(array.shape)]
        where[longest] = (where[longest] + shift) % array.shape[longest]
        spots.append(tuple(where))
    return array.at[spots[0]].set(low).at[spots[1]].set(top_value)


def steps_of(own_key, dims, cuts, low, high):
    gain, own = 1.0, jax.random.fold_in(own_key, 6)
    for axis_at, blocks in cuts:
        heights = jnp.exp(jax.random.uniform(jax.random.fold_in(own, axis_at), (blocks,), jnp.float32, low / len(cuts), high / len(cuts)))
        gain = gain * jnp.repeat(heights, dims[axis_at] // blocks).reshape([-1 if axis == axis_at else 1 for axis in range(len(dims))])
    return gain


def assign_block(rng, own, number, rows, number_of, top, most, skew):
    ranking = jax.random.permutation(rng, number_of)
    packed, common = load_shares(number_of, rows * top, most, skew, True), load_shares(number_of, rows * top, most, skew, False)
    places = jnp.arange(number_of)

    def named(sizes, rotation):
        used = int((sizes > 0).sum())
        fixed = max(1, used // 4)
        moved = fixed + (places - fixed + rotation * (used - fixed)) % max(1, number_of - fixed)
        return jnp.zeros((number_of,), jnp.int32).at[ranking[jnp.where(places < fixed, places, moved)]].set(jnp.asarray(sizes, jnp.int32))

    sizes = jnp.where(number % 4 == 0, named(packed, number // 4), named(common, number - number // 4 - 1))
    mixed = jax.random.permutation(jax.random.fold_in(own, 3), number_of)
    source_of, taker = mixed[0:number_of // 2 * 2:2], mixed[1:number_of // 2 * 2:2]
    slack = jnp.minimum(sizes[source_of] - 1, most - sizes[taker]) // 2
    slack = jnp.where((source_of == ranking[0]) | (taker == ranking[0]) | (sizes[taker] == 0), 0, jnp.maximum(slack, 0))
    moved = jax.random.randint(jax.random.fold_in(own, 4), (number_of // 2,), 0, 1 << 20) % (slack + 1)
    sizes = sizes.at[source_of].add(-moved).at[taker].add(moved)
    members = jnp.searchsorted(jnp.cumsum(sizes), jnp.arange(rows * top), side="right").astype(jnp.int32)
    grid = members.reshape(top, rows).T
    grid = grid[jax.random.permutation(jax.random.fold_in(own, 1), rows)]
    rotation = jax.random.randint(jax.random.fold_in(own, 2), (rows, 1), 0, top)
    return jnp.take_along_axis(grid, (jnp.arange(top)[None, :] + rotation) % top, axis=1)


def load_shares(count, total, most, slope, full):
    portions = [(1 << 20) // math.isqrt(rank ** slope) + 1 for rank in range(1, count + 1)]
    largest = most if full else min(most, max(-(-total // count), total * portions[0] // sum(portions)))
    least = 1 if total - largest >= count - 1 else 0
    given, rest = [largest] + [least] * (count - 1), total - largest - least * (count - 1)
    while rest > 0:
        candidates = [i for i in range(1, count) if given[i] < largest] or [i for i in range(1, count) if given[i] < most]
        pool, remaining = sum([portions[i] for i in candidates]), rest
        for i in candidates:
            addition = min(most - given[i], max(1, remaining * portions[i] // pool), rest)
            given[i] = given[i] + addition
            rest = rest - addition
    return np.array(given)


def bell_draw(own_key, shape, deviation, reach, pieces=(), held_as=jnp.bfloat16):
    level = steps_of(own_key, shape, pieces, -0.22, 0.18) if pieces else 1.0
    entries = jax.random.normal(own_key, shape, jnp.float32) * deviation * level
    return jnp.minimum(jnp.maximum(entries, -reach), reach).astype(held_as)


def setup_inputs(seed: int = 0) -> dict:
    key_list = jax.random.split(jax.random.key(seed), 27)
    tokens = bell_draw(key_list[0], (SEQS, D), 1.0, 6.0, ((0, 32),))
    lengths = plant(jax.random.randint(key_list[1], (SEQS,), LEN // 16, LEN + 1), jax.random.fold_in(key_list[1], 1), LEN // 16, LEN).astype(jnp.int32)
    cache_latent = bell_draw(key_list[2], (SEQS, LEN, LATENT), 1.0, 6.0, ((0, 32),))
    cache_rope_key = draw_cache_rope_key(jax.random.fold_in(key_list[26], 71), 0)
    route_ids_keys = jax.random.split(jax.random.fold_in(key_list[4], 1), SEQS // GROUP)
    route_ids_turns = jax.random.permutation(jax.random.fold_in(key_list[4], 3), SEQS // GROUP)
    route_ids = jax.vmap(lambda own, number: assign_block(jax.random.fold_in(key_list[4], 2), own, number, GROUP, EXPERTS, TOP_K, CAP, 2))(route_ids_keys, route_ids_turns).reshape((SEQS, TOP_K))
    route_weights = jnp.clip(jnp.exp(math.log(2.0) - 2.3025851 * jax.random.uniform(key_list[5], (SEQS, TOP_K), jnp.float32) ** steps_of(key_list[5], (SEQS, TOP_K), ((0, 4),), -0.2, 0.2)), 0.2, 2.0)
    attn_gain = jnp.clip(1.0 + 0.18 * jax.random.normal(key_list[6], (D,), jnp.float32), 0.1, 1.9)
    w_query_nope = bell_draw(key_list[7], (D, HEADS, NOPE), D ** -0.5, 0.125, ((1, 8),))
    w_query_rope = bell_draw(key_list[8], (D, HEADS, ROPE), D ** -0.5, 0.125, ((1, 8),))
    w_latent_down = bell_draw(key_list[9], (D, LATENT), D ** -0.5, 0.125, ((1, 8),))
    w_key_rope = bell_draw(key_list[10], (D, ROPE), D ** -0.5, 0.125)
    latent_gain = jnp.clip(1.0 + 0.18 * jax.random.normal(key_list[11], (LATENT,), jnp.float32), 0.1, 1.9)
    w_key_up = bell_draw(key_list[12], (LATENT, HEADS, NOPE), NOPE ** -0.5, 0.75, ((1, 8),))
    w_value_up = bell_draw(key_list[13], (LATENT, HEADS, VHEAD), LATENT ** -0.5, 0.25, ((1, 8),))
    w_attn_out = bell_draw(key_list[14], (HEADS, VHEAD, D), (HEADS * VHEAD) ** -0.5, 0.1875, ((0, 8),))
    ffn_gain = jnp.clip(1.0 + 0.18 * jax.random.normal(key_list[15], (D,), jnp.float32), 0.1, 1.9)
    expert_gate = bell_draw(key_list[16], (EXPERTS, D, EXPERT_FF), D ** -0.5, 0.125, ((0, 32),))
    expert_up = bell_draw(key_list[17], (EXPERTS, D, EXPERT_FF), D ** -0.5, 0.125, ((0, 32),))
    expert_down = bell_draw(key_list[18], (EXPERTS, EXPERT_FF, D), EXPERT_FF ** -0.5, 0.25, ((0, 32),))
    shared_gate = bell_draw(key_list[19], (D, SHARED_FF), D ** -0.5, 0.125, ((1, 8),))
    shared_up = bell_draw(key_list[20], (D, SHARED_FF), D ** -0.5, 0.125, ((1, 8),))
    shared_down = bell_draw(key_list[21], (SHARED_FF, D), SHARED_FF ** -0.5, 0.25, ((0, 8),))
    dense_gate = bell_draw(key_list[22], (D, DENSE_FF), D ** -0.5, 0.125, ((1, 8),))
    dense_up = bell_draw(key_list[23], (D, DENSE_FF), D ** -0.5, 0.125, ((1, 8),))
    dense_down = bell_draw(key_list[24], (DENSE_FF, D), DENSE_FF ** -0.5, 0.1875, ((0, 8),))
    branch_gate = bell_draw(key_list[25], (D,), D ** -0.5, 0.125)
    return dict(tokens=tokens, lengths=lengths, cache_latent=cache_latent, cache_rope_key=cache_rope_key, route_ids=route_ids, route_weights=route_weights, attn_gain=attn_gain, w_query_nope=w_query_nope, w_query_rope=w_query_rope, w_latent_down=w_latent_down, w_key_rope=w_key_rope, latent_gain=latent_gain, w_key_up=w_key_up, w_value_up=w_value_up, w_attn_out=w_attn_out, ffn_gain=ffn_gain, expert_gate=expert_gate, expert_up=expert_up, expert_down=expert_down, shared_gate=shared_gate, shared_up=shared_up, shared_down=shared_down, dense_gate=dense_gate, dense_up=dense_up, dense_down=dense_down, branch_gate=branch_gate)


epsilon = 1e-06
rope_base = 10000.0

def norm_rows(values, scales):
    values = values.astype(jnp.float32)
    factor = lax.rsqrt(lax.optimization_barrier(jnp.mean(values * values, axis=-1, keepdims=True)) + epsilon)
    return values * factor * scales.astype(jnp.float32)

def rotate(values, positions):
    half_dim = values.shape[-1] // 2
    frequencies = rope_base ** (-jnp.arange(half_dim).astype(jnp.float32) / half_dim)
    angles = positions.astype(jnp.float32)[:, None] * frequencies[None, :]
    bcast_shape = (angles.shape[0],) + (1,) * (values.ndim - 2) + (half_dim,)
    cosine = jnp.cos(angles).reshape(bcast_shape)
    sine_val = jnp.sin(angles).reshape(bcast_shape)
    first_half = values[..., :half_dim].astype(jnp.float32)
    second_half = values[..., half_dim:].astype(jnp.float32)
    return jnp.concatenate([first_half * cosine - second_half * sine_val, first_half * sine_val + second_half * cosine], axis=-1)

def swiglu(inputs, gate_w, up_w):
    gate_val = jnp.dot(inputs, gate_w, preferred_element_type=jnp.float32)
    up_val = jnp.dot(inputs, up_w, preferred_element_type=jnp.float32)
    return (jax.nn.silu(gate_val) * up_val).astype(jnp.bfloat16)

def attend(group_data):
    q_lat, q_rot, lat_new, rope_new, lat_cache, rope_cache, seq_len = group_data
    head_scale = (NOPE + ROPE) ** (-0.5)
    scores = jnp.einsum('bhr,blr->bhl', q_lat.astype(jnp.float32), lat_cache.astype(jnp.float32))
    scores = scores + jnp.einsum('bhe,ble->bhl', q_rot.astype(jnp.float32), rope_cache.astype(jnp.float32))
    scores = scores * head_scale
    in_range = jnp.arange(lat_cache.shape[1], dtype=jnp.int32)[None, None, :] < seq_len[:, None, None]
    scores = jnp.where(in_range, scores, -jnp.inf)
    own_score = jnp.einsum('bhr,br->bh', q_lat.astype(jnp.float32), lat_new.astype(jnp.float32))
    own_score = (own_score + jnp.einsum('bhe,be->bh', q_rot.astype(jnp.float32), rope_new.astype(jnp.float32))) * head_scale
    peak_score = jnp.maximum(lax.optimization_barrier(jnp.max(scores, axis=-1)), own_score)
    past_exp = jnp.exp(scores - peak_score[..., None])
    own_exp = jnp.exp(own_score - peak_score)
    total_exp = lax.optimization_barrier(jnp.sum(past_exp, axis=-1)) + own_exp
    past_weight = (past_exp / total_exp[..., None]).astype(jnp.bfloat16)
    own_weight = (own_exp / total_exp).astype(jnp.bfloat16)
    out_latent = jnp.einsum('bhl,blr->bhr', past_weight.astype(jnp.float32), lat_cache.astype(jnp.float32))
    out_latent = out_latent + own_weight.astype(jnp.float32)[..., None] * lat_new.astype(jnp.float32)[:, None, :]
    return out_latent.astype(jnp.bfloat16)

def reference(tokens, lengths, cache_latent, cache_rope_key, route_ids, route_weights, attn_gain, w_query_nope, w_query_rope, w_latent_down, w_key_rope, latent_gain, w_key_up, w_value_up, w_attn_out, ffn_gain, expert_gate, expert_up, expert_down, shared_gate, shared_up, shared_down, dense_gate, dense_up, dense_down, branch_gate):
    seq_count, model_width = tokens.shape
    head_count = w_query_nope.shape[1]
    normed = norm_rows(tokens, attn_gain).astype(jnp.bfloat16)
    query_nope = jnp.dot(normed, w_query_nope.reshape(model_width, -1), preferred_element_type=jnp.float32)
    query_nope = query_nope.astype(jnp.bfloat16).reshape(seq_count, head_count, -1)
    query_latent = jnp.einsum('shn,rhn->shr', query_nope.astype(jnp.float32), w_key_up.astype(jnp.float32)).astype(jnp.bfloat16)
    query_rope = jnp.dot(normed, w_query_rope.reshape(model_width, -1), preferred_element_type=jnp.float32)
    query_rope = query_rope.astype(jnp.bfloat16).reshape(seq_count, head_count, -1)
    latent_raw = jnp.dot(normed, w_latent_down, preferred_element_type=jnp.float32).astype(jnp.bfloat16)
    new_latent = norm_rows(latent_raw, latent_gain).astype(jnp.bfloat16)
    new_rope = rotate(jnp.dot(normed, w_key_rope, preferred_element_type=jnp.float32), lengths).astype(jnp.bfloat16)
    query_rot = rotate(query_rope, lengths).astype(jnp.bfloat16)
    grouped = tuple((member.reshape((N_EP, GROUP) + member.shape[1:]) for member in (query_latent, query_rot, new_latent, new_rope, cache_latent, cache_rope_key, lengths)))
    out_latent = lax.map(attend, grouped).reshape(seq_count, head_count, -1)
    head_values = jnp.einsum('shr,rhv->shv', out_latent.astype(jnp.float32), w_value_up.astype(jnp.float32)).astype(jnp.bfloat16)
    after_attn = tokens.astype(jnp.float32) + jnp.dot(head_values.reshape(seq_count, -1), w_attn_out.reshape(-1, model_width), preferred_element_type=jnp.float32)
    ffn_in = norm_rows(after_attn, ffn_gain).astype(jnp.bfloat16)
    shared_term = jnp.dot(swiglu(ffn_in, shared_gate, shared_up), shared_down, preferred_element_type=jnp.float32)
    branch_mix = jax.nn.sigmoid(jnp.dot(ffn_in, branch_gate, preferred_element_type=jnp.float32))
    dense_term = branch_mix[:, None] * jnp.dot(swiglu(ffn_in, dense_gate, dense_up), dense_down, preferred_element_type=jnp.float32)
    top_count = route_ids.shape[1]
    flat_expert = route_ids.reshape(-1).astype(jnp.int32)
    flat_row = jnp.arange(seq_count * top_count, dtype=jnp.int32) // top_count
    expert_hits = (flat_expert[:, None] == jnp.arange(EXPERTS, dtype=jnp.int32)[None, :]).astype(jnp.int32)
    expert_hits = expert_hits.reshape(N_EP, GROUP * top_count, EXPERTS)
    earlier = jnp.cumsum(expert_hits, axis=1) - expert_hits
    rank_in = lax.optimization_barrier(jnp.sum(earlier * expert_hits, axis=2)).reshape(-1).astype(jnp.int32)
    slot_index = (flat_row // GROUP * CAP + rank_in).astype(jnp.int32)
    slot_table = jnp.full((EXPERTS, N_EP * CAP), seq_count, jnp.int32).at[flat_expert, slot_index].set(flat_row)
    padded_in = jnp.concatenate([ffn_in, jnp.zeros((1, model_width), jnp.bfloat16)], axis=0)

    def one_expert(expert_data):
        row_ids, gate_w, up_w, down_w = expert_data
        act_val = swiglu(padded_in[row_ids], gate_w, up_w)
        return jnp.dot(act_val, down_w, preferred_element_type=jnp.float32).astype(jnp.bfloat16)
    expert_out = lax.map(one_expert, (slot_table, expert_gate, expert_up, expert_down))
    picked = expert_out[flat_expert, slot_index].astype(jnp.float32).reshape(seq_count, top_count, model_width)
    routed = lax.optimization_barrier(jnp.sum(picked * route_weights.astype(jnp.float32)[:, :, None], axis=1))
    mixed = (after_attn + routed + shared_term + dense_term).astype(jnp.bfloat16)
    return (mixed, new_latent, new_rope)
```

```python
import functools

import jax
import jax.numpy as jnp
import numpy as np
from jax import lax
from jax.experimental import pallas as pl
from jax.experimental.pallas import tpu as pltpu
from jax.sharding import PartitionSpec as P

epsilon = 1e-06
rope_base = 10000.0
lanes = 128
F32 = jnp.float32
BF16 = jnp.bfloat16
MESH = pl.DeviceIdType.MESH


def nn(a, b):
    return lax.dot_general(a, b, (((1,), (0,)), ((), ())), preferred_element_type=F32)


def nt(a, b):
    return lax.dot_general(a, b, (((1,), (1,)), ((), ())), preferred_element_type=F32)


def tn(a, b):
    return lax.dot_general(a, b, (((0,), (0,)), ((), ())), preferred_element_type=F32)


def join(pieces):
    return pieces[0] if len(pieces) == 1 else jnp.concatenate(pieces, axis=0)


def flipped(index, mask, count):
    out = index
    bit = 1
    while bit < count:
        if mask & bit:
            out = out + bit - 2 * bit * (index // bit % 2)
        bit *= 2
    return out


def far_first(me, chips, cores):
    chip, core = me // cores, me % cores
    low = 1 - chip // (chips // 2)
    order = []
    for i in range(chips - 1):
        down = chips - 1 - i
        down = down - (chip - down + chips) // chips
        up = i + (i - chip + chips) // chips
        to = low * down + (1 - low) * up
        for turn_core in range(cores):
            order.append(to * cores + (core + turn_core) % cores)
    for turn_core in range(1, cores):
        order.append(chip * cores + (core + turn_core) % cores)
    return order


def flat(ref):
    return jnp.concatenate([ref[i : i + 1, :] for i in range(ref.shape[0])], axis=1)


def spread(values, count):
    rows = values.shape[0]
    return join(
        [jnp.broadcast_to(values[b : b + 1], (count, values.shape[1])) for b in range(rows)]
    )


def rows_of(ref, count):
    return join([ref[i].astype(F32) for i in range(count)])


def factor_of(values):
    return lax.rsqrt(jnp.mean(values * values, axis=-1, keepdims=True) + epsilon)


def silu(v):
    return v / (1.0 + jnp.exp(-v))


def lane_block(values, column, width):
    base, offset = column // lanes * lanes, column % lanes
    block = values[:, base : base + lanes]
    if offset:
        block = pltpu.roll(block, lanes - offset, 1)
    lane = lax.broadcasted_iota(jnp.int32, block.shape, 1)
    return jnp.where(lane < width, block, 0.0)


def turn(values, cosine, sine, half):
    lane = lax.broadcasted_iota(jnp.int32, values.shape, 1)
    swapped = jnp.where(
        lane < half, -pltpu.roll(values, lanes - half, 1), pltpu.roll(values, half, 1)
    )
    return values * cosine + swapped * sine


def layer(
    sizes,
    h_tokens, h_attn_gain, h_lengths, h_turns, h_ids, h_wts, h_ffn_gain, h_latent_gain, h_branch_gate,
    wqn, wqr, wld, wkr, cl, cr, wku, wvu, wo, sg, su, dg, du, sd, dd, eg, eu, ed,
    mixed, newlat, newrope,
    tokens, attn_gain, lengths, turns, ids, wts, ffn_gain, latent_gain, branch_gate,
    v_in, v_kr, v_cl, v_cr, v_ku, v_vu, v_wo, v_s, v_d, v_sd, v_dd, v_e, v_ed,
    agx, sendq, recvq, sendo, recvo, senda, recva, agf, sende, recve, sendr, recvr, sendf, recvf,
    kr_pad, w_sem, tp_send, tp_recv, ep_send, ep_recv,
):
    T, EP, own, H, nope, rope, latent, cap, scale = sizes
    group = T * own
    R = H * own
    me_t = lax.axis_index("tp")
    me_e = lax.axis_index("ep")
    lat_w = wld.shape[0]

    barrier = pltpu.get_barrier_semaphore()
    for k in range(1, T):
        pl.semaphore_signal(
            barrier, inc=1, device_id=(me_e, flipped(me_t, k, T)), device_id_type=MESH
        )
    for k in range(1, EP):
        pl.semaphore_signal(
            barrier, inc=1, device_id=(flipped(me_e, k, EP), me_t), device_id_type=MESH
        )

    n_q, n_r = H * nope, H * rope
    groups = [
        [(h_tokens, tokens)],
        [(h_attn_gain, attn_gain)],
        [
            (wqn, v_in.at[pl.ds(0, n_q)]),
            (wqr, v_in.at[pl.ds(n_q, n_r)]),
            (wld, v_in.at[pl.ds(n_q + n_r, lat_w)]),
        ],
        [(wkr, v_kr)],
        [(wku, v_ku)],
        [(h_lengths, lengths)],
        [(h_turns, turns)],
        [(h_ids, ids)],
        [(h_wts, wts)],
        [(cl, v_cl)],
        [(cr, v_cr)],
        [(wvu, v_vu)],
        [(wo, v_wo)],
        [(h_latent_gain, latent_gain)],
        [(h_ffn_gain, ffn_gain)],
        [(sg, v_s.at[0]), (su, v_s.at[1])],
        [(dg, v_d.at[0]), (du, v_d.at[1])],
        [(sd, v_sd)],
        [(dd, v_dd)],
        [(h_branch_gate, branch_gate)],
        [(eg, v_e.at[0]), (eu, v_e.at[1])],
        [(ed, v_ed)],
    ]
    wholes = {2: v_in, 15: v_s, 16: v_d, 20: v_e}
    first_small, first_cl, first_ffn = 2, 9, 15
    loads = []
    for i, bunch in enumerate(groups):
        for source, target in bunch:
            load = pltpu.make_async_copy(source, target, w_sem.at[i])
            load.start()
        if len(bunch) > 1:
            load = pltpu.make_async_copy(wholes[i], wholes[i], w_sem.at[i])
        loads.append(load)

    sends = []

    order = far_first(me_t, T // 2, 2)

    def tp_exchange(phase, source, target):
        for peer in order:
            pltpu.make_async_remote_copy(
                src_ref=source(peer),
                dst_ref=target.at[me_t],
                send_sem=tp_send.at[phase],
                recv_sem=tp_recv.at[phase],
                device_id=(me_e, peer),
                device_id_type=MESH,
            ).start()
        blocks = target.at[pl.ds(0, T - 1)]
        every = pltpu.make_async_remote_copy(
            src_ref=blocks,
            dst_ref=blocks,
            send_sem=tp_send.at[phase],
            recv_sem=tp_recv.at[phase],
            device_id=(me_e, order[0]),
            device_id_type=MESH,
        )
        sends.append(every)
        return every

    def ep_exchange(phase, source, target):
        for k in range(EP - 1, 0, -1):
            peer = flipped(me_e, k, EP)
            pltpu.make_async_remote_copy(
                src_ref=source.at[peer],
                dst_ref=target.at[me_e],
                send_sem=ep_send.at[phase],
                recv_sem=ep_recv.at[phase],
                device_id=(peer, me_t),
                device_id_type=MESH,
            ).start()
        blocks = target.at[pl.ds(0, EP - 1)]
        every = pltpu.make_async_remote_copy(
            src_ref=blocks,
            dst_ref=blocks,
            send_sem=ep_send.at[phase],
            recv_sem=ep_recv.at[phase],
            device_id=(flipped(me_e, 1, EP), me_t),
            device_id_type=MESH,
        )
        sends.append(every)
        return every

    def arrive(step):
        step.wait_recv()

    for i in range(first_small):
        loads[i].wait()
    x = tokens[...].astype(F32)
    normed = (x * factor_of(x) * flat(attn_gain[...])).astype(BF16)
    agx[me_t] = normed
    pl.semaphore_wait(barrier, T - 1 + EP - 1)
    step = tp_exchange(0, lambda peer: agx.at[me_t], agx)
    for i in range(first_small, first_cl):
        loads[i].wait()

    slots = EP * cap
    slot = lax.broadcasted_iota(jnp.int32, (slots, group), 0)
    block = jnp.zeros((slots, group), jnp.int32)
    for j in range(1, EP):
        block = block + jnp.where(slot >= j * cap, 1, 0)
    expert = block * T + me_t
    place = (slot - block * cap).astype(F32)
    hit = jnp.zeros((slots, group), F32)
    weight = jnp.zeros((slots, group), F32)
    for k in range(ids.shape[0]):
        same = ids[k : k + 1, :] == expert
        hit = hit + jnp.where(same, 1.0, 0.0)
        weight = weight + jnp.where(same, wts[k : k + 1, :], 0.0)
    upper = jnp.where(
        lax.broadcasted_iota(jnp.int32, (group, group), 0)
        < lax.broadcasted_iota(jnp.int32, (group, group), 1),
        1.0,
        0.0,
    ).astype(BF16)
    rank = nn(hit.astype(BF16), upper)
    dispatch = jnp.where(rank == place, hit, 0.0)
    weight = weight * dispatch
    weight_hi = weight.astype(BF16)
    weight_lo = (weight - weight_hi.astype(F32)).astype(BF16)
    dispatch = dispatch.astype(BF16)

    left = jnp.zeros((own, lanes), jnp.int32)
    row = lax.broadcasted_iota(jnp.int32, (own, lanes), 0)
    for b in range(own):
        left = jnp.where(row == b, lengths[b], left)
    length = left
    bits = turns.shape[0] // 2
    cosine = jnp.ones((own, lanes), F32)
    sine = jnp.zeros((own, lanes), F32)
    for i in range(bits - 1, -1, -1):
        has = left >= 2**i
        left = jnp.where(has, left - 2**i, left)
        c, s = turns[i : i + 1, :], turns[bits + i : bits + i + 1, :]
        cosine, sine = (
            jnp.where(has, cosine * c - sine * s, cosine),
            jnp.where(has, cosine * s + sine * c, sine),
        )
    live = lax.broadcasted_iota(jnp.int32, (own, lanes), 1) < rope
    cosine = jnp.where(live, cosine, 0.0)
    sine = jnp.where(live, sine, 0.0)
    big = T * H
    seq = lax.broadcasted_iota(jnp.int32, (own * big, lanes), 0) % own

    def tiled(values):
        return join([values] * big)

    mine = [seq == b for b in range(own)]
    length = tiled(length)
    cosines, sines = tiled(cosine), tiled(sine)
    kr_pad[...] = jnp.zeros_like(kr_pad)
    kr_pad[:, 0:rope] = nt(normed, v_kr[...])
    new_rope = turn(kr_pad[...], cosine, sine, rope // 2).astype(BF16)
    newrope[...] = new_rope[:, 0:rope]

    arrive(step)
    rows = rows_of(agx, T).astype(BF16)
    wide = v_in.shape[0] // 2
    proj = jnp.concatenate(
        [nt(rows, v_in[0:wide, :]), nt(rows, v_in[wide : 2 * wide, :])], axis=1
    )
    q_lat = [
        nn(lane_block(proj, h * nope, nope)[:, 0:nope].astype(BF16), v_ku[h]) for h in range(H)
    ]
    q_rope = [lane_block(proj, n_q + h * rope, rope) for h in range(H)]
    lat_part = pltpu.roll(lane_block(proj, n_q + n_r, lat_w), lanes - lat_w, 1)
    for u in range(T):
        cut = slice(own * u, own * (u + 1))
        sendq[u, :, 0:latent] = join([q[cut] for q in q_lat]).astype(BF16)
        sendq[u, :, latent : latent + lanes] = join(
            [q[cut] + lat_part[cut] for q in q_rope]
        ).astype(BF16)
    step = tp_exchange(1, lambda peer: sendq.at[peer], recvq)
    recvq[me_t] = sendq[me_t]
    for i in range(first_cl, first_ffn):
        loads[i].wait()
    arrive(step)

    queries = rows_of(recvq, T)
    per = lanes // lat_w
    lane = lax.broadcasted_iota(jnp.int32, (own, lanes), 1)
    blocks = []
    for j in range(T // per):
        total = None
        for i in range(per):
            top = R * (j * per + i)
            piece = jnp.where(lane >= lanes - lat_w, queries[top : top + own, latent:], 0.0)
            if i < per - 1:
                piece = pltpu.roll(piece, (i + 1) * lat_w, 1)
            total = piece if total is None else total + piece
        blocks.append(total)
    raw = blocks[0] if len(blocks) == 1 else jnp.concatenate(blocks, axis=1)
    new_latent = (raw * factor_of(raw) * flat(latent_gain[...])).astype(BF16)
    newlat[...] = new_latent
    new_lat32, new_rope32 = new_latent.astype(F32), new_rope.astype(F32)
    q_rot = turn(
        jnp.where(
            lax.broadcasted_iota(jnp.int32, (own * big, lanes), 1) < rope, queries[:, latent:], 0.0
        ),
        cosines,
        sines,
        rope // 2,
    ).astype(BF16).astype(F32)
    q_lat32 = queries[:, 0:latent]
    new_lat_all = tiled(new_lat32)
    own_score = (
        jnp.sum(q_lat32 * new_lat_all, axis=-1, keepdims=True)
        + jnp.sum(q_rot * tiled(new_rope32), axis=-1, keepdims=True)
    ) * scale
    across = None
    wide_q = []
    for b in range(own):
        q_b = jnp.where(mine[b][:, 0:1], q_lat32, 0.0).astype(BF16)
        wide_q.append(q_b)
        turned = pltpu.roll(q_rot, rope * b, 1) if b else q_rot
        turned = jnp.where(mine[b], turned, 0.0)
        across = turned if across is None else across + turned
    across = across[:, 0 : own * rope].astype(BF16)
    wide_q = jnp.concatenate(wide_q, axis=1)
    if own * big < lanes:
        wide_q = join([wide_q, jnp.zeros((lanes - own * big, own * latent), BF16)])
    depth = v_cl.shape[1] // 2
    scores = []
    for part in range(2):
        cut = slice(part * depth, (part + 1) * depth)
        keys = jnp.concatenate([v_cl[b, cut, :] for b in range(own)], axis=1)
        scores.append(nt(keys, wide_q).T[0 : own * big] + nn(across, v_cr[:, cut]))
    scores = jnp.concatenate(scores, axis=1)
    position = lax.broadcasted_iota(jnp.int32, scores.shape, 1)
    scores = jnp.where(position < length[:, 0:1], scores * scale, -jnp.inf)
    peak = jnp.maximum(jnp.max(scores, axis=-1, keepdims=True), own_score)
    past = jnp.exp(scores - peak)
    own_exp = jnp.exp(own_score - peak)
    total = jnp.sum(past, axis=-1, keepdims=True) + own_exp
    past = past / total
    own_weight = (own_exp / total).astype(BF16).astype(F32)
    past = [jnp.where(mine[b][:, 0:1], past, 0.0).astype(BF16) for b in range(own)]
    mixed_lat = []
    for part in range(2):
        cut = slice(part * latent // 2, (part + 1) * latent // 2)
        total = None
        for b in range(own):
            term = nn(past[b], v_cl[b, :, cut])
            total = term if total is None else total + term
        mixed_lat.append(total)
    mixed_lat = jnp.concatenate(mixed_lat, axis=1)
    mixed_lat = mixed_lat + own_weight * new_lat_all
    for u in range(T):
        sendo[u] = mixed_lat[R * u : R * (u + 1)].astype(BF16)
    step = tp_exchange(2, lambda peer: sendo.at[peer], recvo)
    recvo[me_t] = sendo[me_t]
    arrive(step)

    back = rows_of(recvo, T).astype(BF16)
    values = []
    for h in range(H):
        value = nt(back, v_vu[h])
        values.append(
            join([value[R * u + own * h : R * u + own * (h + 1)] for u in range(T)])
        )
    values = values[0] if H == 1 else jnp.concatenate(values, axis=1)
    values = values.astype(BF16)
    wide = v_wo.shape[1] // 2
    part = jnp.concatenate(
        [nn(values, v_wo[:, 0:wide]), nn(values, v_wo[:, wide : 2 * wide])], axis=1
    )
    for u in range(T):
        senda[u] = part[own * u : own * (u + 1)].astype(BF16)
    step = tp_exchange(3, lambda peer: senda.at[peer], recva)
    recva[me_t] = senda[me_t]
    arrive(step)
    after = tokens[...].astype(F32)
    for u in range(T):
        after = after + recva[u].astype(F32)
    agf[me_t] = (after * factor_of(after) * flat(ffn_gain[...])).astype(BF16)
    step = tp_exchange(4, lambda peer: agf.at[me_t], agf)
    for i in range(first_ffn, len(loads)):
        loads[i].wait()
    arrive(step)

    rows32 = rows_of(agf, T)
    rows = rows32.astype(BF16)
    outgoing = nn(dispatch, rows)
    for j in range(EP):
        sende[j] = outgoing[cap * j : cap * (j + 1)].astype(BF16)
    step = ep_exchange(0, sende, recve)
    recve[me_e] = sende[me_e]

    act = (silu(nt(rows, v_s[0])) * nt(rows, v_s[1])).astype(BF16)
    ffn = nn(act, v_sd[...])
    gate = jnp.sum(rows32 * flat(branch_gate[...].astype(F32)), axis=-1, keepdims=True)
    gate = 1.0 / (1.0 + jnp.exp(-gate))
    act = (silu(nn(rows, v_d[0])) * nn(rows, v_d[1])).astype(BF16)
    ffn = ffn + gate * nn(act, v_dd[...])

    arrive(step)
    routed = rows_of(recve, EP).astype(BF16)
    act = (silu(nn(routed, v_e[0])) * nn(routed, v_e[1])).astype(BF16)
    wide = v_ed.shape[1] // 2
    cuts = [slice(0, wide), slice(wide, 2 * wide)]
    steps = []
    for n, cut in enumerate(cuts):
        result = nn(act, v_ed[:, cut])
        for j in range(EP):
            sendr[n, j] = result[cap * j : cap * (j + 1)].astype(BF16)
        steps.append(ep_exchange(1 + n, sendr.at[n], recvr.at[n]))
        recvr[n, me_e] = sendr[n, me_e]
    last = []
    for n, cut in enumerate(cuts):
        arrive(steps[n])
        returned = rows_of(recvr.at[n], EP).astype(BF16)
        part = ffn[:, cut] + (tn(weight_hi, returned) + tn(weight_lo, returned))
        for u in range(T):
            sendf[n, u] = part[own * u : own * (u + 1)].astype(BF16)
        last.append(tp_exchange(5 + n, lambda peer: sendf.at[n, peer], recvf.at[n]))
        recvf[n, me_t] = sendf[n, me_t]
    for n, cut in enumerate(cuts):
        arrive(last[n])
        part = after[:, cut]
        for u in range(T):
            part = part + recvf[n, u].astype(F32)
        mixed[:, cut] = part.astype(BF16)
    for c in sends:
        c.wait_send()


def hand_over(*refs):
    half = len(refs) // 2
    for source, target in zip(refs[:half], refs[half:]):
        target[...] = source[...]


def local(
    tokens, lengths, cache_latent, cache_rope_key, route_ids, route_weights, attn_gain,
    w_query_nope, w_query_rope, w_latent_down, w_key_rope, latent_gain, w_key_up, w_value_up,
    w_attn_out, ffn_gain, expert_gate, expert_up, expert_down, shared_gate, shared_up,
    shared_down, dense_gate, dense_up, dense_down, branch_gate,
):
    own, width = tokens.shape
    T = lax.axis_size("tp")
    EP = lax.axis_size("ep")
    H, nope = w_query_nope.shape[1:]
    rope = w_query_rope.shape[2]
    latent = cache_latent.shape[2]
    top = route_ids.shape[1]
    assert expert_gate.shape[0] == 1
    cap = max(2, (2 * own * top + EP - 1) // EP)
    R = H * own
    half = rope // 2

    bits = cache_latent.shape[1].bit_length()
    frequencies = (rope_base ** (-np.arange(half) / half)).astype(np.float32).astype(np.float64)
    angles = frequencies[None, :] * 2.0 ** np.arange(bits)[:, None]
    angles = np.pad(np.tile(angles, (1, 2)), ((0, 0), (0, lanes - rope)))
    turns = jnp.asarray(np.concatenate([np.cos(angles), np.sin(angles)]), F32)

    operands = (
        tokens,
        attn_gain.reshape(-1, lanes),
        lengths,
        turns,
        route_ids.T,
        route_weights.T,
        ffn_gain.reshape(-1, lanes),
        latent_gain.reshape(-1, lanes),
        branch_gate.reshape(-1, lanes),
        w_query_nope.transpose(1, 2, 0).reshape(H * nope, width),
        w_query_rope.transpose(1, 2, 0).reshape(H * rope, width),
        w_latent_down.T,
        w_key_rope.T,
        cache_latent,
        cache_rope_key.transpose(0, 2, 1).reshape(own * rope, -1),
        w_key_up.transpose(1, 2, 0),
        w_value_up.transpose(1, 2, 0),
        w_attn_out.reshape(-1, width),
        shared_gate.T,
        shared_up.T,
        dense_gate,
        dense_up,
        shared_down,
        dense_down,
        expert_gate[0],
        expert_up[0],
        expert_down[0],
    )
    big = operands[9:]
    v_in = pltpu.VMEM((sum(o.shape[0] for o in big[:3]), width), BF16)
    weights = [v_in] + [
        pltpu.VMEM(shape, BF16)
        for shape in [o.shape for o in big[3:9]]
        + [(2,) + o.shape for o in (big[9], big[11])]
        + [big[13].shape, big[14].shape, (2,) + big[15].shape, big[17].shape]
    ]
    small = [
        (pltpu.SMEM if o is lengths else pltpu.VMEM)(o.shape, o.dtype) for o in operands[:9]
    ]
    q_width = latent + lanes

    def comm(*shape):
        return pltpu.VMEM(shape, BF16)

    buffers = [
        comm(T, own, width),
        comm(T, R, q_width), comm(T, R, q_width),
        comm(T, R, latent), comm(T, R, latent),
        comm(T, own, width), comm(T, own, width),
        comm(T, own, width),
        comm(EP, cap, width), comm(EP, cap, width),
        comm(2, EP, cap, width // 2), comm(2, EP, cap, width // 2),
        comm(2, T, own, width // 2), comm(2, T, own, width // 2),
        pltpu.VMEM((own, lanes), F32),
    ]
    n_loads = 22
    sems = [
        pltpu.SemaphoreType.DMA((n_loads,)),
        pltpu.SemaphoreType.DMA((7,)),
        pltpu.SemaphoreType.DMA((7,)),
        pltpu.SemaphoreType.DMA((3,)),
        pltpu.SemaphoreType.DMA((3,)),
    ]
    sizes = (T, EP, own, H, nope, rope, latent, cap, (nope + rope) ** (-0.5))
    vmem = pl.BlockSpec(memory_space=pltpu.VMEM)
    shapes = [((own, width), BF16), ((own, latent), BF16), ((own, rope), BF16)]
    results = pl.pallas_call(
        functools.partial(layer, sizes),
        out_shape=tuple(pltpu.VMEM(*shape) for shape in shapes),
        in_specs=[pl.BlockSpec(memory_space=pl.ANY)] * len(operands),
        out_specs=(vmem, vmem, vmem),
        scratch_shapes=small + weights + buffers + sems,
        compiler_params=pltpu.CompilerParams(collective_id=0, has_side_effects=True),
    )(*operands)
    return pl.pallas_call(
        hand_over,
        out_shape=tuple(jax.ShapeDtypeStruct(*shape) for shape in shapes),
        in_specs=[vmem] * 3,
        out_specs=(vmem, vmem, vmem),
    )(*[pltpu.with_memory_space_constraint(r, pltpu.VMEM) for r in results])


def solution(mesh):
    both = ("ep", "tp")
    in_specs = (
        P(both, None),
        P(both),
        P(both, None, None),
        P(both, None, None),
        P("ep", None),
        P("ep", None),
        P(),
        P(None, "tp", None),
        P(None, "tp", None),
        P(None, "tp"),
        P(),
        P(),
        P(None, "tp", None),
        P(None, "tp", None),
        P("tp", None, None),
        P(),
        P(both, None, None),
        P(both, None, None),
        P(both, None, None),
        P(None, "tp"),
        P(None, "tp"),
        P("tp", None),
        P(None, "tp"),
        P(None, "tp"),
        P("tp", None),
        P(),
    )
    out_specs = (P(both, None), P(both, None), P(both, None))
    return jax.shard_map(local, mesh=mesh, in_specs=in_specs, out_specs=out_specs, check_vma=False)
```

```python
import functools

import jax
import jax.numpy as jnp
import numpy as np
from jax import lax
from jax.experimental import pallas as pl
from jax.experimental.pallas import tpu as pltpu
from jax.sharding import PartitionSpec as P

epsilon = 1e-06
rope_base = 10000.0
lanes = 128
F32 = jnp.float32
BF16 = jnp.bfloat16
MESH = pl.DeviceIdType.MESH


def nn(a, b):
    return lax.dot_general(a, b, (((1,), (0,)), ((), ())), preferred_element_type=F32)


def nt(a, b):
    return lax.dot_general(a, b, (((1,), (1,)), ((), ())), preferred_element_type=F32)


def tn(a, b):
    return lax.dot_general(a, b, (((0,), (0,)), ((), ())), preferred_element_type=F32)


def join(pieces):
    return pieces[0] if len(pieces) == 1 else jnp.concatenate(pieces, axis=0)


def flipped(index, mask, count):
    out = index
    bit = 1
    while bit < count:
        if mask & bit:
            out = out + bit - 2 * bit * (index // bit % 2)
        bit *= 2
    return out


def far_first(chip, chips):
    low = 1 - chip // (chips // 2)
    order = []
    for i in range(chips - 1):
        down = chips - 1 - i
        down = down - (chip - down + chips) // chips
        up = i + (i - chip + chips) // chips
        order.append(low * down + (1 - low) * up)
    return order


def flat(ref):
    return jnp.concatenate([ref[i : i + 1, :] for i in range(ref.shape[0])], axis=1)


def spread(values, count):
    rows = values.shape[0]
    return join(
        [jnp.broadcast_to(values[b : b + 1], (count, values.shape[1])) for b in range(rows)]
    )


def rows_of(ref, count):
    return join([ref[i].astype(F32) for i in range(count)])


def factor_of(values):
    return lax.rsqrt(jnp.mean(values * values, axis=-1, keepdims=True) + epsilon)


def in_three(value):
    lane = lax.broadcasted_iota(jnp.int32, (value.shape[0], lanes), 1)
    out = jnp.zeros(lane.shape, F32)
    for i in range(3):
        part = value.astype(BF16).astype(F32)
        out = jnp.where(lane == i, part, out)
        value = value - part
    return out.astype(BF16)


def scaled(halves):
    half = halves[0].shape[1] - lanes
    total = jnp.sum(halves[0][:, half:] + halves[1][:, half:], axis=-1, keepdims=True)
    factor = lax.rsqrt(total / (2 * half) + epsilon)
    return jnp.concatenate([(h[:, 0:half] * factor).astype(BF16) for h in halves], axis=1)


def silu(v):
    return v / (1.0 + jnp.exp(-v))


def turn(values, cosine, sine, half):
    lane = lax.broadcasted_iota(jnp.int32, values.shape, 1)
    swapped = jnp.where(
        lane < half, -pltpu.roll(values, lanes - half, 1), pltpu.roll(values, half, 1)
    )
    return values * cosine + swapped * sine


def layer(
    sizes,
    h_tokens, h_attn_gain, h_lengths, h_turns, h_ids, h_wts, h_ffn_gain, h_latent_gain, h_branch_gate,
    wqn, wqr, wld, wkr, cl, cr, wku, wvu, wo, sg, su, dg, du, sd, dd, eg, eu, ed,
    mixed, newlat, newrope,
    toks, attn_gain, lengths, turns, ids, wts, ffn_gain, latent_gain, branch_gate,
    v_in, v_kr, v_cl, v_cr, v_ku, v_vu, v_wo, v_s, v_d, v_sd, v_dd, v_e, v_ed,
    agx, sendq, recvq, sendo, recvo, senda, recva, half_after, after, agf, halves,
    sende, recve, ffn_own, ffn_other, sendr, recvr, sendf, recvf,
    kr_pad, w_sem, tp_send, tp_recv, ep_send, ep_recv, pair_send, pair_recv,
):
    T, EP, own, H, nope, rope, latent, cap, scale = sizes
    group = T * own
    R = H * own
    me_t = lax.axis_index("tp")
    me_e = lax.axis_index("ep")
    lat_w = wld.shape[0]

    Z = T // 2
    me_z, me_k = me_t // 2, me_t % 2
    partner = me_t + 1 - 2 * me_k
    width = agx.shape[2]
    half = width // 2
    chips = far_first(me_z, Z)
    order = []
    for z in chips:
        order += [2 * z + me_k, 2 * z + 1 - me_k]
    order.append(partner)

    barrier = pltpu.get_barrier_semaphore()
    for peer in order:
        pl.semaphore_signal(barrier, inc=1, device_id=(me_e, peer), device_id_type=MESH)
    for k in range(1, EP):
        for peer in (me_t, partner):
            pl.semaphore_signal(
                barrier, inc=1, device_id=(flipped(me_e, k, EP), peer), device_id_type=MESH
            )

    n_q, n_r = H * nope, H * rope
    groups = [
        [(h_tokens, toks.at[me_k])],
        [(h_attn_gain, attn_gain)],
        [
            (wqn, v_in.at[me_k, pl.ds(0, n_q)]),
            (wqr, v_in.at[me_k, pl.ds(n_q, n_r)]),
            (wld, v_in.at[me_k, pl.ds(n_q + n_r, lat_w)]),
        ],
        [(wkr, v_kr)],
        [(wku, v_ku.at[me_k])],
        [(h_lengths, lengths)],
        [(h_turns, turns)],
        [(h_ids, ids)],
        [(h_wts, wts)],
        [(cl, v_cl)],
        [(cr, v_cr)],
        [(wvu, v_vu.at[me_k])],
        [(wo, v_wo.at[me_k])],
        [(h_latent_gain, latent_gain)],
        [(h_ffn_gain, ffn_gain)],
        [(sg, v_s.at[0]), (su, v_s.at[1])],
        [(dg, v_d.at[0]), (du, v_d.at[1])],
        [(sd, v_sd)],
        [(dd, v_dd)],
        [(h_branch_gate, branch_gate)],
        [(eg, v_e.at[0]), (eu, v_e.at[1])],
        [(ed, v_ed)],
    ]
    wholes = {2: v_in.at[me_k], 15: v_s, 16: v_d, 20: v_e}
    first_small, first_cl, first_ffn = 2, 9, 15
    loads = []
    for i, bunch in enumerate(groups):
        for source, target in bunch:
            load = pltpu.make_async_copy(source, target, w_sem.at[i])
            load.start()
        if len(bunch) > 1:
            load = pltpu.make_async_copy(wholes[i], wholes[i], w_sem.at[i])
        loads.append(load)

    sends = []

    def remote(source, target, send_sem, recv_sem, e, t):
        return pltpu.make_async_remote_copy(
            src_ref=source,
            dst_ref=target,
            send_sem=send_sem,
            recv_sem=recv_sem,
            device_id=(e, t),
            device_id_type=MESH,
        )

    def whole(blocks, send_sem, recv_sem):
        every = remote(blocks, blocks, send_sem, recv_sem, me_e, partner)
        sends.append(every)
        return every

    def tp_exchange(phase, source, target):
        sems = tp_send.at[phase], tp_recv.at[phase]
        for peer in order:
            remote(source(peer), target.at[me_t], *sems, me_e, peer).start()
        return whole(target.at[pl.ds(0, T - 1)], *sems)

    def chip_exchange(phase, source, target, core):
        sems = tp_send.at[phase], tp_recv.at[phase]
        for z in chips:
            remote(source(z), target.at[me_z], *sems, me_e, 2 * z + core).start()
        return whole(target.at[pl.ds(0, Z - 1)], *sems)

    def ep_exchange(phase, source, target):
        sems = ep_send.at[phase], ep_recv.at[phase]
        for k in range(EP - 1, 0, -1):
            peer = flipped(me_e, k, EP)
            for c, t in ((me_k, me_t), (1 - me_k, partner)):
                remote(source.at[2 * peer + c], target.at[2 * me_e + me_k], *sems, peer, t).start()
        mine = 2 * me_e + me_k
        remote(source.at[2 * me_e + 1 - me_k], target.at[mine], *sems, me_e, partner).start()
        target[mine] = source[mine]
        return whole(target.at[pl.ds(0, 2 * EP - 1)], *sems)

    def pair_copy(i, source, target):
        copy = remote(source, target, pair_send.at[i], pair_recv.at[i], me_e, partner)
        copy.start()
        sends.append(copy)
        return copy

    def arrive(step):
        step.wait_recv()

    for i in range(first_small):
        loads[i].wait()
    x = toks[me_k].astype(F32)
    normed = (x * factor_of(x) * flat(attn_gain[...])).astype(BF16)
    agx[me_z] = normed
    pl.semaphore_wait(barrier, T - 1 + 2 * (EP - 1))
    step = chip_exchange(0, lambda z: agx.at[me_z], agx, 1 - me_k)
    for i in range(first_small, first_cl):
        loads[i].wait()
    early = [
        pair_copy(6, v_in.at[me_k], v_in.at[me_k]),
        pair_copy(7, v_ku.at[me_k], v_ku.at[me_k]),
    ]

    slots = EP * 2 * cap
    slot = lax.broadcasted_iota(jnp.int32, (slots, group), 0)
    block = slot // cap
    expert = block // 2 * T + block % 2 + 2 * me_z
    place = (slot - block * cap).astype(F32)
    hit = jnp.zeros((slots, group), F32)
    weight = jnp.zeros((slots, group), F32)
    for k in range(ids.shape[0]):
        same = ids[k : k + 1, :] == expert
        hit = hit + jnp.where(same, 1.0, 0.0)
        weight = weight + jnp.where(same, wts[k : k + 1, :], 0.0)
    upper = jnp.where(
        lax.broadcasted_iota(jnp.int32, (group, group), 0)
        < lax.broadcasted_iota(jnp.int32, (group, group), 1),
        1.0,
        0.0,
    ).astype(BF16)
    rank = nn(hit.astype(BF16), upper)
    dispatch = jnp.where(rank == place, hit, 0.0)
    weight = weight * dispatch
    weight_hi = weight.astype(BF16)
    weight_lo = (weight - weight_hi.astype(F32)).astype(BF16)
    dispatch = dispatch.astype(BF16)

    left = jnp.zeros((own, lanes), jnp.int32)
    row = lax.broadcasted_iota(jnp.int32, (own, lanes), 0)
    for b in range(own):
        left = jnp.where(row == b, lengths[b], left)
    length = left
    bits = turns.shape[0] // 2
    cosine = jnp.ones((own, lanes), F32)
    sine = jnp.zeros((own, lanes), F32)
    for i in range(bits - 1, -1, -1):
        has = left >= 2**i
        left = jnp.where(has, left - 2**i, left)
        c, s = turns[i : i + 1, :], turns[bits + i : bits + i + 1, :]
        cosine, sine = (
            jnp.where(has, cosine * c - sine * s, cosine),
            jnp.where(has, cosine * s + sine * c, sine),
        )
    live = lax.broadcasted_iota(jnp.int32, (own, lanes), 1) < rope
    cosine = jnp.where(live, cosine, 0.0)
    sine = jnp.where(live, sine, 0.0)
    big = T * H
    seq = lax.broadcasted_iota(jnp.int32, (own * big, lanes), 0) % own

    def tiled(values):
        return join([values] * big)

    mine = [seq == b for b in range(own)]
    length = tiled(length)
    cosines, sines = tiled(cosine), tiled(sine)
    kr_pad[...] = jnp.zeros_like(kr_pad)
    kr_pad[:, 0:rope] = nt(normed, v_kr[...])
    new_rope = turn(kr_pad[...], cosine, sine, rope // 2).astype(BF16)
    newrope[...] = new_rope[:, 0:rope]

    for copy in early:
        arrive(copy)
    arrive(step)
    rows = rows_of(agx, Z).astype(BF16)
    count = rows.shape[0]
    lane = lax.broadcasted_iota(jnp.int32, (count, n_q), 1) // nope
    spare = jnp.zeros((lanes - rope - lat_w, count), F32)
    q_lat, q_rope = [], []
    projected = [nt(v_in[c], rows) for c in range(2)]
    for c, proj in enumerate(projected):
        every = proj[0:n_q].T
        every = join([jnp.where(lane == h, every, 0.0) for h in range(H)]).astype(BF16)
        every = nn(every, join([v_ku[c, h] for h in range(H)]))
        q_lat += [every[count * h : count * (h + 1)] for h in range(H)]
        for h in range(H):
            top = n_q + h * rope
            q_rope.append(join([proj[top : top + rope], spare, proj[n_q + n_r :]]).T)
    for z in range(Z):
        cut = slice(own * z, own * (z + 1))
        sendq[z, :, 0:latent] = join([q[cut] for q in q_lat]).astype(BF16)
        sendq[z, :, latent : latent + lanes] = join([q[cut] for q in q_rope]).astype(BF16)
    step = chip_exchange(1, lambda z: sendq.at[z], recvq, 1 - me_k)
    recvq[me_z] = sendq[me_z]
    shared = [
        pair_copy(0, toks.at[me_k], toks.at[me_k]),
        pair_copy(1, wvu, v_vu.at[me_k]),
        pair_copy(2, wo, v_wo.at[me_k]),
    ]
    for i in range(first_cl, first_ffn):
        loads[i].wait()
    arrive(step)

    queries = rows_of(recvq, Z)
    per = lanes // lat_w
    lane = lax.broadcasted_iota(jnp.int32, (own, lanes), 1)
    blocks = []
    for j in range(T // per):
        total = None
        for i in range(per):
            top = R * (j * per + i)
            piece = jnp.where(lane >= lanes - lat_w, queries[top : top + own, latent:], 0.0)
            if i < per - 1:
                piece = pltpu.roll(piece, (i + 1) * lat_w, 1)
            total = piece if total is None else total + piece
        blocks.append(total)
    raw = blocks[0] if len(blocks) == 1 else jnp.concatenate(blocks, axis=1)
    new_latent = (raw * factor_of(raw) * flat(latent_gain[...])).astype(BF16)
    newlat[...] = new_latent
    new_lat32, new_rope32 = new_latent.astype(F32), new_rope.astype(F32)
    q_rot = turn(
        jnp.where(
            lax.broadcasted_iota(jnp.int32, (own * big, lanes), 1) < rope, queries[:, latent:], 0.0
        ),
        cosines,
        sines,
        rope // 2,
    ).astype(BF16).astype(F32)
    q_lat32 = queries[:, 0:latent]
    new_lat_all = tiled(new_lat32)
    own_score = (
        jnp.sum(q_lat32 * new_lat_all, axis=-1, keepdims=True)
        + jnp.sum(q_rot * tiled(new_rope32), axis=-1, keepdims=True)
    ) * scale
    across = None
    wide_q = []
    for b in range(own):
        q_b = jnp.where(mine[b][:, 0:1], q_lat32, 0.0).astype(BF16)
        wide_q.append(q_b)
        turned = pltpu.roll(q_rot, rope * b, 1) if b else q_rot
        turned = jnp.where(mine[b], turned, 0.0)
        across = turned if across is None else across + turned
    across = across[:, 0 : own * rope].astype(BF16)
    wide_q = jnp.concatenate(wide_q, axis=1)
    depth = v_cl.shape[1] // 2
    scores = []
    for part in range(2):
        cut = slice(part * depth, (part + 1) * depth)
        keys = jnp.concatenate([v_cl[b, cut, :] for b in range(own)], axis=1)
        scores.append(nt(keys, wide_q).T + nn(across, v_cr[:, cut]))
    scores = jnp.concatenate(scores, axis=1)
    position = lax.broadcasted_iota(jnp.int32, scores.shape, 1)
    scores = jnp.where(position < length[:, 0:1], scores * scale, -jnp.inf)
    peak = jnp.maximum(jnp.max(scores, axis=-1, keepdims=True), own_score)
    past = jnp.exp(scores - peak)
    own_exp = jnp.exp(own_score - peak)
    total = jnp.sum(past, axis=-1, keepdims=True) + own_exp
    past = past / total
    own_weight = (own_exp / total).astype(BF16).astype(F32)
    past = [jnp.where(mine[b][:, 0:1], past, 0.0).astype(BF16) for b in range(own)]
    mixed_lat = []
    for part in range(2):
        cut = slice(part * latent // 2, (part + 1) * latent // 2)
        total = None
        for b in range(own):
            term = nn(past[b], v_cl[b, :, cut])
            total = term if total is None else total + term
        mixed_lat.append(total)
    mixed_lat = jnp.concatenate(mixed_lat, axis=1)
    mixed_lat = mixed_lat + own_weight * new_lat_all
    for z in range(Z):
        sendo[z] = mixed_lat[2 * R * z : 2 * R * (z + 1)].astype(BF16)
    step = chip_exchange(2, lambda z: sendo.at[z], recvo, 1 - me_k)
    recvo[me_z] = sendo[me_z]
    for copy in shared:
        arrive(copy)
    arrive(step)

    back = rows_of(recvo, Z).astype(BF16)
    value = nt(back, join([v_vu[0], v_vu[1]]))
    heads = 2 * H
    vhead = value.shape[1] // heads
    at_head = lax.broadcasted_iota(jnp.int32, value.shape, 0) // own % heads
    of_head = lax.broadcasted_iota(jnp.int32, value.shape, 1) // vhead
    value = jnp.where(at_head == of_head, value, 0.0)
    values = []
    for z in range(Z):
        total = None
        for q in range(heads):
            top = own * (heads * z + q)
            term = value[top : top + own]
            total = term if total is None else total + term
        values.append(total)
    values = join(values).astype(BF16)
    for c in range(2):
        cut = slice(c * half, (c + 1) * half)
        part = nn(values, join([v_wo[0, :, cut], v_wo[1, :, cut]]))
        for z in range(Z):
            senda[2 * z + c] = part[own * z : own * (z + 1)].astype(BF16)
    step = tp_exchange(3, lambda peer: senda.at[peer], recva)
    recva[me_t] = senda[me_t]
    arrive(step)
    here = pl.ds(pl.multiple_of(me_k * half, lanes), half)
    eight = []
    for c in range(2):
        total = toks[c, :, here].astype(F32) + recva[2 * me_z + c].astype(F32)
        for z in chips:
            total = total + recva[2 * z + 1 - c].astype(F32)
        half_after[c] = total
        eight.append(total)
    eight = join(eight)
    tiles = half // lanes
    gain = jnp.concatenate(
        [ffn_gain[pl.ds(me_k * tiles + i, 1), :] for i in range(tiles)], axis=1
    )
    agf[me_z, :, 0:half] = (eight * gain).astype(BF16)
    agf[me_z, :, half:] = in_three(jnp.sum(eight * eight, axis=-1, keepdims=True))
    step = chip_exchange(4, lambda z: agf.at[me_z], agf, me_k)
    after_copy = pair_copy(3, half_after.at[1 - me_k], after.at[me_k])
    after[me_k] = half_after[me_k]
    for i in range(first_ffn, len(loads)):
        loads[i].wait()
    arrive(step)

    unscaled = rows_of(agf, Z).astype(BF16)
    halves[me_k] = unscaled
    outgoing = nn(dispatch, unscaled)
    for j in range(2 * EP):
        sende[j] = outgoing[cap * j : cap * (j + 1)].astype(BF16)
    step = ep_exchange(0, sende, recve)
    arrive(pair_copy(4, halves.at[me_k], halves.at[me_k]))
    rows = scaled([halves[c].astype(F32) for c in range(2)])
    rows32 = rows.astype(F32)
    act = (silu(nt(rows, v_s[0])) * nt(rows, v_s[1])).astype(BF16)
    ffn = nn(act, v_sd[...])
    gate = jnp.sum(rows32 * flat(branch_gate[...].astype(F32)), axis=-1, keepdims=True)
    gate = 1.0 / (1.0 + jnp.exp(-gate))
    act = (silu(nn(rows, v_d[0])) * nn(rows, v_d[1])).astype(BF16)
    ffn = ffn + gate * nn(act, v_dd[...])

    for c in range(2):
        ffn_own[c] = ffn[:, c * half : (c + 1) * half]
    ffn_copy = pair_copy(5, ffn_own.at[1 - me_k], ffn_other)

    arrive(step)
    routed = scaled([join([recve[2 * j + c].astype(F32) for j in range(EP)]) for c in range(2)])
    act = (silu(nn(routed, v_e[0])) * nn(routed, v_e[1])).astype(BF16)
    pieces = sendr.shape[0]
    wide = half // pieces
    steps = []
    for n in range(pieces):
        for c in range(2):
            base = c * half + n * wide
            result = nn(act, v_ed[:, base : base + wide])
            for j in range(EP):
                sendr[n, 2 * j + c] = result[cap * j : cap * (j + 1)].astype(BF16)
        steps.append(ep_exchange(1 + n, sendr.at[n], recvr.at[n]))
    arrive(ffn_copy)
    arrive(after_copy)
    ffn = ffn_own[me_k] + ffn_other[...]
    last = []
    for n in range(pieces):
        arrive(steps[n])
        returned = rows_of(recvr.at[n], 2 * EP).astype(BF16)
        part = ffn[:, n * wide : (n + 1) * wide]
        part = part + (tn(weight_hi, returned) + tn(weight_lo, returned))
        for u in range(T):
            sendf[n, u] = part[own * u : own * (u + 1)].astype(BF16)
        last.append(tp_exchange(5 + n, lambda peer: sendf.at[n, peer], recvf.at[n]))
        recvf[n, me_t] = sendf[n, me_t]
    for n in range(pieces):
        arrive(last[n])
        for c in range(2):
            part = after[c, :, n * wide : (n + 1) * wide]
            for z in range(Z):
                part = part + recvf[n, 2 * z + c].astype(F32)
            base = c * half + n * wide
            mixed[:, base : base + wide] = part.astype(BF16)
    for c in sends:
        c.wait_send()


def hand_over(*refs):
    half = len(refs) // 2
    for source, target in zip(refs[:half], refs[half:]):
        target[...] = source[...]


def local(
    tokens, lengths, cache_latent, cache_rope_key, route_ids, route_weights, attn_gain,
    w_query_nope, w_query_rope, w_latent_down, w_key_rope, latent_gain, w_key_up, w_value_up,
    w_attn_out, ffn_gain, expert_gate, expert_up, expert_down, shared_gate, shared_up,
    shared_down, dense_gate, dense_up, dense_down, branch_gate,
):
    own, width = tokens.shape
    T = lax.axis_size("tp")
    EP = lax.axis_size("ep")
    H, nope = w_query_nope.shape[1:]
    rope = w_query_rope.shape[2]
    latent = cache_latent.shape[2]
    top = route_ids.shape[1]
    assert expert_gate.shape[0] == 1
    cap = max(2, (2 * own * top + EP - 1) // EP)
    R = H * own
    half = rope // 2

    bits = cache_latent.shape[1].bit_length()
    frequencies = (rope_base ** (-np.arange(half) / half)).astype(np.float32).astype(np.float64)
    angles = frequencies[None, :] * 2.0 ** np.arange(bits)[:, None]
    angles = np.pad(np.tile(angles, (1, 2)), ((0, 0), (0, lanes - rope)))
    turns = jnp.asarray(np.concatenate([np.cos(angles), np.sin(angles)]), F32)

    operands = (
        tokens,
        attn_gain.reshape(-1, lanes),
        lengths,
        turns,
        route_ids.T,
        route_weights.T,
        ffn_gain.reshape(-1, lanes),
        latent_gain.reshape(-1, lanes),
        branch_gate.reshape(-1, lanes),
        w_query_nope.transpose(1, 2, 0).reshape(H * nope, width),
        w_query_rope.transpose(1, 2, 0).reshape(H * rope, width),
        w_latent_down.T,
        w_key_rope.T,
        cache_latent,
        cache_rope_key.transpose(0, 2, 1).reshape(own * rope, -1),
        w_key_up.transpose(1, 2, 0),
        w_value_up.transpose(1, 2, 0).reshape(-1, latent),
        w_attn_out.reshape(-1, width),
        shared_gate.T,
        shared_up.T,
        dense_gate,
        dense_up,
        shared_down,
        dense_down,
        expert_gate[0],
        expert_up[0],
        expert_down[0],
    )
    big = operands[9:]
    v_in = pltpu.VMEM((2, sum(o.shape[0] for o in big[:3]), width), BF16)
    pair = (2,)
    weights = [v_in] + [
        pltpu.VMEM(shape, BF16)
        for shape in [o.shape for o in big[3:6]]
        + [pair + o.shape for o in (big[6], big[7], big[8], big[9], big[11])]
        + [big[13].shape, big[14].shape, pair + big[15].shape, big[17].shape]
    ]
    small = [pltpu.VMEM((2, own, width), BF16)] + [
        (pltpu.SMEM if o is lengths else pltpu.VMEM)(o.shape, o.dtype) for o in operands[1:9]
    ]
    q_width = latent + lanes

    def comm(*shape):
        return pltpu.VMEM(shape, BF16)

    half, chips, group, pieces = width // 2, T // 2, T * own, 2
    buffers = [
        comm(chips, own, width),
        comm(chips, 2 * R, q_width), comm(chips, 2 * R, q_width),
        comm(chips, 2 * R, latent), comm(chips, 2 * R, latent),
        comm(T, own, half), comm(T, own, half),
        pltpu.VMEM((2, own, half), F32), pltpu.VMEM((2, own, half), F32),
        comm(chips, 2 * own, half + lanes),
        comm(2, group, half + lanes),
        comm(2 * EP, cap, half + lanes), comm(2 * EP, cap, half + lanes),
        pltpu.VMEM((2, group, half), F32), pltpu.VMEM((group, half), F32),
        comm(pieces, 2 * EP, cap, half // pieces), comm(pieces, 2 * EP, cap, half // pieces),
        comm(pieces, T, own, half // pieces), comm(pieces, T, own, half // pieces),
        pltpu.VMEM((own, lanes), F32),
    ]
    n_loads = 22
    sems = [
        pltpu.SemaphoreType.DMA((n_loads,)),
        pltpu.SemaphoreType.DMA((7,)),
        pltpu.SemaphoreType.DMA((7,)),
        pltpu.SemaphoreType.DMA((3,)),
        pltpu.SemaphoreType.DMA((3,)),
        pltpu.SemaphoreType.DMA((8,)),
        pltpu.SemaphoreType.DMA((8,)),
    ]
    sizes = (T, EP, own, H, nope, rope, latent, cap, (nope + rope) ** (-0.5))
    vmem = pl.BlockSpec(memory_space=pltpu.VMEM)
    shapes = [((own, width), BF16), ((own, latent), BF16), ((own, rope), BF16)]
    results = pl.pallas_call(
        functools.partial(layer, sizes),
        out_shape=tuple(pltpu.VMEM(*shape) for shape in shapes),
        in_specs=[pl.BlockSpec(memory_space=pl.ANY)] * len(operands),
        out_specs=(vmem, vmem, vmem),
        scratch_shapes=small + weights + buffers + sems,
        compiler_params=pltpu.CompilerParams(collective_id=0, has_side_effects=True),
    )(*operands)
    return pl.pallas_call(
        hand_over,
        out_shape=tuple(jax.ShapeDtypeStruct(*shape) for shape in shapes),
        in_specs=[vmem] * 3,
        out_specs=(vmem, vmem, vmem),
    )(*[pltpu.with_memory_space_constraint(r, pltpu.VMEM) for r in results])


def solution(mesh):
    both = ("ep", "tp")
    in_specs = (
        P(both, None),
        P(both),
        P(both, None, None),
        P(both, None, None),
        P("ep", None),
        P("ep", None),
        P(),
        P(None, "tp", None),
        P(None, "tp", None),
        P(None, "tp"),
        P(),
        P(),
        P(None, "tp", None),
        P(None, "tp", None),
        P("tp", None, None),
        P(),
        P(both, None, None),
        P(both, None, None),
        P(both, None, None),
        P(None, "tp"),
        P(None, "tp"),
        P("tp", None),
        P(None, "tp"),
        P(None, "tp"),
        P("tp", None),
        P(),
    )
    out_specs = (P(both, None), P(both, None), P(both, None))
    return jax.shard_map(local, mesh=mesh, in_specs=in_specs, out_specs=out_specs, check_vma=False)
```

```python
import functools

import jax
import jax.numpy as jnp
import numpy as np
from jax import lax
from jax.experimental import pallas as pl
from jax.experimental.pallas import tpu as pltpu
from jax.sharding import PartitionSpec as P

epsilon = 1e-06
rope_base = 10000.0
lanes = 128
F32 = jnp.float32
BF16 = jnp.bfloat16
MESH = pl.DeviceIdType.MESH


def nn(a, b):
    return lax.dot_general(a, b, (((1,), (0,)), ((), ())), preferred_element_type=F32)


def nt(a, b):
    return lax.dot_general(a, b, (((1,), (1,)), ((), ())), preferred_element_type=F32)


def tn(a, b):
    return lax.dot_general(a, b, (((0,), (0,)), ((), ())), preferred_element_type=F32)


def join(pieces):
    return pieces[0] if len(pieces) == 1 else jnp.concatenate(pieces, axis=0)


def flipped(index, mask, count):
    out = index
    bit = 1
    while bit < count:
        if mask & bit:
            out = out + bit - 2 * bit * (index // bit % 2)
        bit *= 2
    return out


def far_first(chip, chips):
    low = 1 - chip // (chips // 2)
    order = []
    for i in range(chips - 1):
        down = chips - 1 - i
        down = down - (chip - down + chips) // chips
        up = i + (i - chip + chips) // chips
        order.append(low * down + (1 - low) * up)
    return order


def flat(ref):
    return jnp.concatenate([ref[i : i + 1, :] for i in range(ref.shape[0])], axis=1)


def spread(values, count):
    rows = values.shape[0]
    return join(
        [jnp.broadcast_to(values[b : b + 1], (count, values.shape[1])) for b in range(rows)]
    )


def rows_of(ref, count):
    return join([ref[i].astype(F32) for i in range(count)])


def factor_of(values):
    return lax.rsqrt(jnp.mean(values * values, axis=-1, keepdims=True) + epsilon)


def silu(v):
    return v / (1.0 + jnp.exp(-v))


def turn(values, cosine, sine, half):
    lane = lax.broadcasted_iota(jnp.int32, values.shape, 1)
    swapped = jnp.where(
        lane < half, -pltpu.roll(values, lanes - half, 1), pltpu.roll(values, half, 1)
    )
    return values * cosine + swapped * sine


def layer(
    sizes,
    h_tokens, h_attn_gain, h_lengths, h_turns, h_ids, h_wts, h_ffn_gain, h_latent_gain, h_branch_gate,
    wqn, wqr, wld, wkr, cl, cr, wku, wvu, wo, sg, su, dg, du, sd, dd, eg, eu, ed,
    mixed, newlat, newrope,
    tokens, attn_gain, lengths, turns, ids, wts, ffn_gain, latent_gain, branch_gate,
    v_in, v_kr, v_cl, v_cr, v_ku, v_vu, v_wo, v_s, v_d, v_sd, v_dd, v_e, v_ed,
    agx, sendq, recvq, sendo, recvo, senda, recva, sendg, agf, halves,
    sende, recve, ffn_own, ffn_other, sendr, recvr, sendf, recvf,
    kr_pad, by_row, v_it, v_ct, w_sem, tp_send, tp_recv, ep_send, ep_recv, pair_send, pair_recv,
):
    T, EP, own, H, nope, rope, latent, cap, scale = sizes
    group = T * own
    R = H * own
    me_t = lax.axis_index("tp")
    me_e = lax.axis_index("ep")
    lat_w = wld.shape[0]

    Z = T // 2
    me_z, me_k = me_t // 2, me_t % 2
    partner = me_t + 1 - 2 * me_k
    width = agx.shape[2]
    half = width // 2
    chips = far_first(me_z, Z)
    order = []
    for z in chips:
        order += [2 * z + me_k, 2 * z + 1 - me_k]
    order.append(partner)

    barrier = pltpu.get_barrier_semaphore()
    for peer in order:
        pl.semaphore_signal(barrier, inc=1, device_id=(me_e, peer), device_id_type=MESH)
    for k in range(1, EP):
        for peer in (me_t, partner):
            pl.semaphore_signal(
                barrier, inc=1, device_id=(flipped(me_e, k, EP), peer), device_id_type=MESH
            )

    n_q, n_r = H * nope, H * rope
    groups = [
        [(h_tokens, tokens)],
        [(h_attn_gain, attn_gain)],
        [
            (wqn, v_in.at[pl.ds(0, n_q)]),
            (wqr, v_in.at[pl.ds(n_q, n_r)]),
            (wld, v_in.at[pl.ds(n_q + n_r, lat_w)]),
        ],
        [(wkr, v_kr)],
        [(wku, v_ku.at[me_k])],
        [(h_lengths, lengths)],
        [(h_turns, turns)],
        [(h_ids, ids)],
        [(h_wts, wts)],
        [(cl, v_cl)],
        [(cr, v_cr)],
        [(wvu, v_vu.at[me_k])],
        [(wo, v_wo.at[me_k])],
        [(h_latent_gain, latent_gain)],
        [(h_ffn_gain, ffn_gain)],
        [(sg, v_s.at[0]), (su, v_s.at[1])],
        [(dg, v_d.at[0]), (du, v_d.at[1])],
        [(sd, v_sd)],
        [(dd, v_dd)],
        [(h_branch_gate, branch_gate)],
        [(eg, v_e.at[0]), (eu, v_e.at[1])],
        [(ed, v_ed)],
    ]
    wholes = {2: v_in, 15: v_s, 16: v_d, 20: v_e}
    first_small, first_cl, first_ffn = 2, 9, 15
    loads = []
    for i, bunch in enumerate(groups):
        for source, target in bunch:
            load = pltpu.make_async_copy(source, target, w_sem.at[i])
            load.start()
        if len(bunch) > 1:
            load = pltpu.make_async_copy(wholes[i], wholes[i], w_sem.at[i])
        loads.append(load)

    sends = []

    def remote(source, target, send_sem, recv_sem, e, t):
        return pltpu.make_async_remote_copy(
            src_ref=source,
            dst_ref=target,
            send_sem=send_sem,
            recv_sem=recv_sem,
            device_id=(e, t),
            device_id_type=MESH,
        )

    def whole(blocks, send_sem, recv_sem):
        every = remote(blocks, blocks, send_sem, recv_sem, me_e, partner)
        sends.append(every)
        return every

    def tp_exchange(phase, source, target):
        sems = tp_send.at[phase], tp_recv.at[phase]
        for peer in order:
            remote(source(peer), target.at[me_t], *sems, me_e, peer).start()
        return whole(target.at[pl.ds(0, T - 1)], *sems)

    def chip_exchange(phase, source, target, core):
        sems = tp_send.at[phase], tp_recv.at[phase]
        for z in chips:
            remote(source(z), target.at[me_z], *sems, me_e, 2 * z + core).start()
        return whole(target.at[pl.ds(0, Z - 1)], *sems)

    def ep_exchange(phase, source, target):
        sems = ep_send.at[phase], ep_recv.at[phase]
        for k in range(EP - 1, 0, -1):
            peer = flipped(me_e, k, EP)
            for c, t in ((me_k, me_t), (1 - me_k, partner)):
                remote(source.at[2 * peer + c], target.at[2 * me_e + me_k], *sems, peer, t).start()
        mine = 2 * me_e + me_k
        remote(source.at[2 * me_e + 1 - me_k], target.at[mine], *sems, me_e, partner).start()
        target[mine] = source[mine]
        return whole(target.at[pl.ds(0, 2 * EP - 1)], *sems)

    def pair_copy(i, source, target):
        copy = remote(source, target, pair_send.at[i], pair_recv.at[i], me_e, partner)
        copy.start()
        sends.append(copy)
        return copy

    def arrive(step):
        step.wait_recv()

    for i in range(first_small):
        loads[i].wait()
    x = tokens[...].astype(F32)
    normed = (x * factor_of(x) * flat(attn_gain[...])).astype(BF16)
    agx[me_z] = normed
    loads[2].wait()
    strip = 2 * lanes

    def turn_weights(i, carry):
        at = pl.ds(pl.multiple_of(i * strip, strip), strip)
        v_it[me_k, at, :] = v_in[:, at].T
        return carry

    lax.fori_loop(0, width // strip, turn_weights, 0)
    pl.semaphore_wait(barrier, T - 1 + 2 * (EP - 1))
    step = chip_exchange(0, lambda z: agx.at[me_z], agx, 1 - me_k)
    for i in range(first_small + 1, first_cl):
        loads[i].wait()
    early = [
        pair_copy(4, v_it.at[me_k], v_it.at[me_k]),
        pair_copy(5, v_ku.at[me_k], v_ku.at[me_k]),
    ]

    slots = EP * 2 * cap
    slot = lax.broadcasted_iota(jnp.int32, (slots, group), 0)
    block = slot // cap
    expert = block // 2 * T + block % 2 + 2 * me_z
    place = (slot - block * cap).astype(F32)
    hit = jnp.zeros((slots, group), F32)
    weight = jnp.zeros((slots, group), F32)
    for k in range(ids.shape[0]):
        same = ids[k : k + 1, :] == expert
        hit = hit + jnp.where(same, 1.0, 0.0)
        weight = weight + jnp.where(same, wts[k : k + 1, :], 0.0)
    upper = jnp.where(
        lax.broadcasted_iota(jnp.int32, (group, group), 0)
        < lax.broadcasted_iota(jnp.int32, (group, group), 1),
        1.0,
        0.0,
    ).astype(BF16)
    rank = nn(hit.astype(BF16), upper)
    dispatch = jnp.where(rank == place, hit, 0.0)
    weight = weight * dispatch
    weight_hi = weight.astype(BF16)
    weight_lo = (weight - weight_hi.astype(F32)).astype(BF16)
    dispatch = dispatch.astype(BF16)

    left = jnp.zeros((own, lanes), jnp.int32)
    row = lax.broadcasted_iota(jnp.int32, (own, lanes), 0)
    for b in range(own):
        left = jnp.where(row == b, lengths[b], left)
    length = left
    bits = turns.shape[0] // 2
    cosine = jnp.ones((own, lanes), F32)
    sine = jnp.zeros((own, lanes), F32)
    for i in range(bits - 1, -1, -1):
        has = left >= 2**i
        left = jnp.where(has, left - 2**i, left)
        c, s = turns[i : i + 1, :], turns[bits + i : bits + i + 1, :]
        cosine, sine = (
            jnp.where(has, cosine * c - sine * s, cosine),
            jnp.where(has, cosine * s + sine * c, sine),
        )
    live = lax.broadcasted_iota(jnp.int32, (own, lanes), 1) < rope
    cosine = jnp.where(live, cosine, 0.0)
    sine = jnp.where(live, sine, 0.0)
    big = T * H
    seq = lax.broadcasted_iota(jnp.int32, (own * big, lanes), 0) // big
    mine = [seq == b for b in range(own)]
    length = spread(length, big)
    cosines, sines = spread(cosine, big), spread(sine, big)
    kr_pad[...] = jnp.zeros_like(kr_pad)
    kr_pad[:, 0:rope] = nt(normed, v_kr[...])
    new_rope = turn(kr_pad[...], cosine, sine, rope // 2).astype(BF16)
    newrope[...] = new_rope[:, 0:rope]

    for copy in early:
        arrive(copy)
    arrive(step)
    rows = rows_of(agx, Z).astype(BF16)
    count = rows.shape[0]
    of_head = lax.broadcasted_iota(jnp.int32, (count, n_q), 1) // nope
    lane = lax.broadcasted_iota(jnp.int32, (count, lanes), 1)
    q_lat, q_rope = [], []
    projected = [nn(rows, v_it[c]) for c in range(2)]
    for c, proj in enumerate(projected):
        every = join([jnp.where(of_head == h, proj[:, 0:n_q], 0.0) for h in range(H)])
        every = nn(every.astype(BF16), join([v_ku[c, h] for h in range(H)]))
        q_lat += [every[count * h : count * (h + 1)] for h in range(H)]
        tail = proj[:, proj.shape[1] - lanes :]
        lat_part = jnp.where(lane >= lanes - lat_w, tail, 0.0)
        for h in range(H):
            offset = n_q + h * rope - (proj.shape[1] - lanes)
            piece = pltpu.roll(tail, lanes - offset, 1) if offset else tail
            q_rope.append(jnp.where(lane < rope, piece, lat_part))
    for z in range(Z):
        cut = slice(own * z, own * (z + 1))
        sendq[z, :, 0:latent] = join([q[cut] for q in q_lat]).astype(BF16)
        sendq[z, :, latent : latent + lanes] = join([q[cut] for q in q_rope]).astype(BF16)
    step = chip_exchange(1, lambda z: sendq.at[z], recvq, 1 - me_k)
    recvq[me_z] = sendq[me_z]
    for i in range(first_cl, first_ffn):
        loads[i].wait()

    per_step = 256

    def turn_keys(i, carry):
        b = i // (v_cl.shape[1] // per_step)
        at = pl.ds(pl.multiple_of(i % (v_cl.shape[1] // per_step) * per_step, lanes), per_step)
        v_ct[b, :, at] = v_cl[b, at, :].T
        return carry

    lax.fori_loop(0, own * (v_cl.shape[1] // per_step), turn_keys, 0)

    arrive(step)
    shared = [
        pair_copy(0, v_vu.at[me_k], v_vu.at[me_k]),
        pair_copy(1, v_wo.at[me_k], v_wo.at[me_k]),
    ]

    queries = rows_of(recvq, Z)
    per = lanes // lat_w
    lane = lax.broadcasted_iota(jnp.int32, (own, lanes), 1)
    blocks = []
    for j in range(T // per):
        total = None
        for i in range(per):
            top = R * (j * per + i)
            piece = jnp.where(lane >= lanes - lat_w, queries[top : top + own, latent:], 0.0)
            if i < per - 1:
                piece = pltpu.roll(piece, (i + 1) * lat_w, 1)
            total = piece if total is None else total + piece
        blocks.append(total)
    raw = blocks[0] if len(blocks) == 1 else jnp.concatenate(blocks, axis=1)
    new_latent = (raw * factor_of(raw) * flat(latent_gain[...])).astype(BF16)
    newlat[...] = new_latent
    new_lat32, new_rope32 = new_latent.astype(F32), new_rope.astype(F32)
    tiles = by_row.shape[0]
    for i in range(tiles):
        by_row[i] = queries[:, lanes * i : lanes * (i + 1)]
    queries = jnp.concatenate(
        [
            join([by_row[i, pl.ds(b, big, stride=own), :] for b in range(own)])
            for i in range(tiles)
        ],
        axis=1,
    )
    q_rot = turn(
        jnp.where(
            lax.broadcasted_iota(jnp.int32, (own * big, lanes), 1) < rope, queries[:, latent:], 0.0
        ),
        cosines,
        sines,
        rope // 2,
    ).astype(BF16).astype(F32)
    q_lat32 = queries[:, 0:latent]
    new_lat_all = spread(new_lat32, big)
    own_score = (
        jnp.sum(q_lat32 * new_lat_all, axis=-1, keepdims=True)
        + jnp.sum(q_rot * spread(new_rope32, big), axis=-1, keepdims=True)
    ) * scale
    across = None
    q_lat16 = q_lat32.astype(BF16)
    for b in range(own):
        turned = pltpu.roll(q_rot, rope * b, 1) if b else q_rot
        turned = jnp.where(mine[b], turned, 0.0)
        across = turned if across is None else across + turned
    across = across[:, 0 : own * rope].astype(BF16)
    depth = v_cl.shape[1] // 2
    scores = []
    for part in range(2):
        cut = slice(part * depth, (part + 1) * depth)
        part = [nn(q_lat16[big * b : big * (b + 1)], v_ct[b, :, cut]) for b in range(own)]
        scores.append(join(part) + nn(across, v_cr[:, cut]))
    scores = jnp.concatenate(scores, axis=1)
    position = lax.broadcasted_iota(jnp.int32, scores.shape, 1)
    scores = jnp.where(position < length[:, 0:1], scores * scale, -jnp.inf)
    peak = jnp.maximum(jnp.max(scores, axis=-1, keepdims=True), own_score)
    past = jnp.exp(scores - peak)
    own_exp = jnp.exp(own_score - peak)
    weights = jnp.sum(past, axis=-1, keepdims=True) + own_exp
    past = past.astype(BF16)
    mixed_lat = []
    for part in range(2):
        cut = slice(part * latent // 2, (part + 1) * latent // 2)
        mixed_lat.append(
            join([nn(past[big * b : big * (b + 1)], v_cl[b, :, cut]) for b in range(own)])
        )
    mixed_lat = jnp.concatenate(mixed_lat, axis=1)
    mixed_lat = (mixed_lat + own_exp * new_lat_all) / weights
    tiles = latent // lanes
    for i in range(tiles):
        for b in range(own):
            block = mixed_lat[big * b : big * (b + 1), lanes * i : lanes * (i + 1)]
            by_row[i, pl.ds(b, big, stride=own), :] = block
    mixed_lat = jnp.concatenate([by_row[i] for i in range(tiles)], axis=1)
    for z in range(Z):
        sendo[z] = mixed_lat[2 * R * z : 2 * R * (z + 1)].astype(BF16)
    step = chip_exchange(2, lambda z: sendo.at[z], recvo, 1 - me_k)
    recvo[me_z] = sendo[me_z]
    for copy in shared:
        arrive(copy)
    arrive(step)

    back = rows_of(recvo, Z).astype(BF16)
    value = jnp.concatenate([nt(back, v_vu[c]) for c in range(2)], axis=1)
    heads = 2 * H
    vhead = value.shape[1] // heads
    at_head = lax.broadcasted_iota(jnp.int32, value.shape, 0) // own % heads
    of_head = lax.broadcasted_iota(jnp.int32, value.shape, 1) // vhead
    value = jnp.where(at_head == of_head, value, 0.0)
    values = []
    for z in range(Z):
        total = None
        for q in range(heads):
            top = own * (heads * z + q)
            term = value[top : top + own]
            total = term if total is None else total + term
        values.append(total)
    values = join(values).astype(BF16)
    for c in range(2):
        cut = slice(c * half, (c + 1) * half)
        part = nn(values, join([v_wo[0, :, cut], v_wo[1, :, cut]]))
        for z in range(Z):
            senda[z, :, cut] = part[own * z : own * (z + 1)].astype(BF16)
    step = chip_exchange(3, lambda z: senda.at[z], recva, 1 - me_k)
    recva[me_z] = senda[me_z]
    arrive(step)
    after = tokens[...].astype(F32)
    for z in range(Z):
        after = after + recva[z].astype(F32)
    normed = (after * factor_of(after) * flat(ffn_gain[...])).astype(BF16)
    for c in range(2):
        sendg[c] = normed[:, c * half : (c + 1) * half]
    step = tp_exchange(4, lambda peer: sendg.at[peer % 2], agf)
    agf[me_t] = sendg[me_k]
    for i in range(first_ffn, len(loads)):
        loads[i].wait()
    arrive(step)

    rows = rows_of(agf, T).astype(BF16)
    halves[me_k] = rows
    outgoing = nn(dispatch, rows)
    for j in range(2 * EP):
        sende[j] = outgoing[cap * j : cap * (j + 1)].astype(BF16)
    step = ep_exchange(0, sende, recve)
    arrive(pair_copy(2, halves.at[me_k], halves.at[me_k]))
    rows = jnp.concatenate([halves[0], halves[1]], axis=1)
    rows32 = rows.astype(F32)
    act = (silu(nt(rows, v_s[0])) * nt(rows, v_s[1])).astype(BF16)
    ffn = nn(act, v_sd[...])
    gate = jnp.sum(rows32 * flat(branch_gate[...].astype(F32)), axis=-1, keepdims=True)
    gate = 1.0 / (1.0 + jnp.exp(-gate))
    act = (silu(nn(rows, v_d[0])) * nn(rows, v_d[1])).astype(BF16)
    ffn = ffn + gate * nn(act, v_dd[...])

    for c in range(2):
        ffn_own[c] = ffn[:, c * half : (c + 1) * half]
    ffn_copy = pair_copy(3, ffn_own.at[1 - me_k], ffn_other)

    arrive(step)
    routed = jnp.concatenate(
        [join([recve[2 * j + c].astype(F32) for j in range(EP)]) for c in range(2)], axis=1
    ).astype(BF16)
    act = (silu(nn(routed, v_e[0])) * nn(routed, v_e[1])).astype(BF16)
    pieces = sendr.shape[0]
    wide = half // pieces
    steps = []
    for n in range(pieces):
        for c in range(2):
            base = c * half + n * wide
            result = nn(act, v_ed[:, base : base + wide])
            for j in range(EP):
                sendr[n, 2 * j + c] = result[cap * j : cap * (j + 1)].astype(BF16)
        steps.append(ep_exchange(1 + n, sendr.at[n], recvr.at[n]))
    arrive(ffn_copy)
    ffn = ffn_own[me_k] + ffn_other[...]
    last = []
    for n in range(pieces):
        arrive(steps[n])
        returned = rows_of(recvr.at[n], 2 * EP).astype(BF16)
        part = ffn[:, n * wide : (n + 1) * wide]
        part = part + (tn(weight_hi, returned) + tn(weight_lo, returned))
        for u in range(T):
            sendf[n, u] = part[own * u : own * (u + 1)].astype(BF16)
        last.append(tp_exchange(5 + n, lambda peer: sendf.at[n, peer], recvf.at[n]))
        recvf[n, me_t] = sendf[n, me_t]
    for n in range(pieces):
        arrive(last[n])
        for c in range(2):
            base = c * half + n * wide
            part = after[:, base : base + wide]
            for z in range(Z):
                part = part + recvf[n, 2 * z + c].astype(F32)
            mixed[:, base : base + wide] = part.astype(BF16)
    for c in sends:
        c.wait_send()


def hand_over(*refs):
    half = len(refs) // 2
    for source, target in zip(refs[:half], refs[half:]):
        target[...] = source[...]


def local(
    tokens, lengths, cache_latent, cache_rope_key, route_ids, route_weights, attn_gain,
    w_query_nope, w_query_rope, w_latent_down, w_key_rope, latent_gain, w_key_up, w_value_up,
    w_attn_out, ffn_gain, expert_gate, expert_up, expert_down, shared_gate, shared_up,
    shared_down, dense_gate, dense_up, dense_down, branch_gate,
):
    own, width = tokens.shape
    T = lax.axis_size("tp")
    EP = lax.axis_size("ep")
    H, nope = w_query_nope.shape[1:]
    rope = w_query_rope.shape[2]
    latent = cache_latent.shape[2]
    top = route_ids.shape[1]
    assert expert_gate.shape[0] == 1
    cap = max(2, (2 * own * top + EP - 1) // EP)
    R = H * own
    half = rope // 2

    bits = cache_latent.shape[1].bit_length()
    frequencies = (rope_base ** (-np.arange(half) / half)).astype(np.float32).astype(np.float64)
    angles = frequencies[None, :] * 2.0 ** np.arange(bits)[:, None]
    angles = np.pad(np.tile(angles, (1, 2)), ((0, 0), (0, lanes - rope)))
    turns = jnp.asarray(np.concatenate([np.cos(angles), np.sin(angles)]), F32)

    operands = (
        tokens,
        attn_gain.reshape(-1, lanes),
        lengths,
        turns,
        route_ids.T,
        route_weights.T,
        ffn_gain.reshape(-1, lanes),
        latent_gain.reshape(-1, lanes),
        branch_gate.reshape(-1, lanes),
        w_query_nope.transpose(1, 2, 0).reshape(H * nope, width),
        w_query_rope.transpose(1, 2, 0).reshape(H * rope, width),
        w_latent_down.T,
        w_key_rope.T,
        cache_latent,
        cache_rope_key.transpose(0, 2, 1).reshape(own * rope, -1),
        w_key_up.transpose(1, 2, 0),
        w_value_up.transpose(1, 2, 0).reshape(-1, latent),
        w_attn_out.reshape(-1, width),
        shared_gate.T,
        shared_up.T,
        dense_gate,
        dense_up,
        shared_down,
        dense_down,
        expert_gate[0],
        expert_up[0],
        expert_down[0],
    )
    big = operands[9:]
    v_in = pltpu.VMEM((sum(o.shape[0] for o in big[:3]), width), BF16)
    pair = (2,)
    weights = [v_in] + [
        pltpu.VMEM(shape, BF16)
        for shape in [o.shape for o in big[3:6]]
        + [pair + o.shape for o in (big[6], big[7], big[8], big[9], big[11])]
        + [big[13].shape, big[14].shape, pair + big[15].shape, big[17].shape]
    ]
    small = [
        (pltpu.SMEM if o is lengths else pltpu.VMEM)(o.shape, o.dtype) for o in operands[:9]
    ]
    q_width = latent + lanes

    def comm(*shape):
        return pltpu.VMEM(shape, BF16)

    half, chips, group, pieces = width // 2, T // 2, T * own, 2
    buffers = [
        comm(chips, own, width),
        comm(chips, 2 * R, q_width), comm(chips, 2 * R, q_width),
        comm(chips, 2 * R, latent), comm(chips, 2 * R, latent),
        comm(chips, own, width), comm(chips, own, width),
        comm(2, own, half),
        comm(T, own, half),
        comm(2, group, half),
        comm(2 * EP, cap, half), comm(2 * EP, cap, half),
        pltpu.VMEM((2, group, half), F32), pltpu.VMEM((group, half), F32),
        comm(pieces, 2 * EP, cap, half // pieces), comm(pieces, 2 * EP, cap, half // pieces),
        comm(pieces, T, own, half // pieces), comm(pieces, T, own, half // pieces),
        pltpu.VMEM((own, lanes), F32),
        pltpu.VMEM((q_width // lanes, T * R, lanes), F32),
        comm(2, width, v_in.shape[0]),
        comm(own, latent, cache_latent.shape[1]),
    ]
    n_loads = 22
    sems = [
        pltpu.SemaphoreType.DMA((n_loads,)),
        pltpu.SemaphoreType.DMA((7,)),
        pltpu.SemaphoreType.DMA((7,)),
        pltpu.SemaphoreType.DMA((3,)),
        pltpu.SemaphoreType.DMA((3,)),
        pltpu.SemaphoreType.DMA((6,)),
        pltpu.SemaphoreType.DMA((6,)),
    ]
    sizes = (T, EP, own, H, nope, rope, latent, cap, (nope + rope) ** (-0.5))
    vmem = pl.BlockSpec(memory_space=pltpu.VMEM)
    shapes = [((own, width), BF16), ((own, latent), BF16), ((own, rope), BF16)]
    results = pl.pallas_call(
        functools.partial(layer, sizes),
        out_shape=tuple(pltpu.VMEM(*shape) for shape in shapes),
        in_specs=[pl.BlockSpec(memory_space=pl.ANY)] * len(operands),
        out_specs=(vmem, vmem, vmem),
        scratch_shapes=small + weights + buffers + sems,
        compiler_params=pltpu.CompilerParams(collective_id=0, has_side_effects=True),
    )(*operands)
    return pl.pallas_call(
        hand_over,
        out_shape=tuple(jax.ShapeDtypeStruct(*shape) for shape in shapes),
        in_specs=[vmem] * 3,
        out_specs=(vmem, vmem, vmem),
    )(*[pltpu.with_memory_space_constraint(r, pltpu.VMEM) for r in results])


def solution(mesh):
    both = ("ep", "tp")
    in_specs = (
        P(both, None),
        P(both),
        P(both, None, None),
        P(both, None, None),
        P("ep", None),
        P("ep", None),
        P(),
        P(None, "tp", None),
        P(None, "tp", None),
        P(None, "tp"),
        P(),
        P(),
        P(None, "tp", None),
        P(None, "tp", None),
        P("tp", None, None),
        P(),
        P(both, None, None),
        P(both, None, None),
        P(both, None, None),
        P(None, "tp"),
        P(None, "tp"),
        P("tp", None),
        P(None, "tp"),
        P(None, "tp"),
        P("tp", None),
        P(),
    )
    out_specs = (P(both, None), P(both, None), P(both, None))
    return jax.shard_map(local, mesh=mesh, in_specs=in_specs, out_specs=out_specs, check_vma=False)
```

```python
import functools

import jax
import jax.numpy as jnp
import numpy as np
from jax import lax
from jax.experimental import pallas as pl
from jax.experimental.pallas import tpu as pltpu
from jax.sharding import PartitionSpec as P

epsilon = 1e-06
rope_base = 10000.0
lanes = 128
F32 = jnp.float32
BF16 = jnp.bfloat16
MESH = pl.DeviceIdType.MESH


def nn(a, b):
    return lax.dot_general(a, b, (((1,), (0,)), ((), ())), preferred_element_type=F32)


def nt(a, b):
    return lax.dot_general(a, b, (((1,), (1,)), ((), ())), preferred_element_type=F32)


def tn(a, b):
    return lax.dot_general(a, b, (((0,), (0,)), ((), ())), preferred_element_type=F32)


def join(pieces):
    return pieces[0] if len(pieces) == 1 else jnp.concatenate(pieces, axis=0)


def flipped(index, mask, count):
    out = index
    bit = 1
    while bit < count:
        if mask & bit:
            out = out + bit - 2 * bit * (index // bit % 2)
        bit *= 2
    return out


def far_first(chip, chips):
    low = 1 - chip // (chips // 2)
    order = []
    for i in range(chips - 1):
        down = chips - 1 - i
        down = down - (chip - down + chips) // chips
        up = i + (i - chip + chips) // chips
        order.append(low * down + (1 - low) * up)
    return order


def flat(ref):
    return jnp.concatenate([ref[i : i + 1, :] for i in range(ref.shape[0])], axis=1)


def spread(values, count):
    rows = values.shape[0]
    return join(
        [jnp.broadcast_to(values[b : b + 1], (count, values.shape[1])) for b in range(rows)]
    )


def rows_of(ref, count):
    return join([ref[i].astype(F32) for i in range(count)])


def factor_of(values):
    return lax.rsqrt(jnp.mean(values * values, axis=-1, keepdims=True) + epsilon)


def silu(v):
    return v / (1.0 + jnp.exp(-v))


def turn(values, cosine, sine, half):
    lane = lax.broadcasted_iota(jnp.int32, values.shape, 1)
    swapped = jnp.where(
        lane < half, -pltpu.roll(values, lanes - half, 1), pltpu.roll(values, half, 1)
    )
    return values * cosine + swapped * sine


def layer(
    sizes,
    h_tokens, h_attn_gain, h_lengths, h_turns, h_ids, h_wts, h_ffn_gain, h_latent_gain, h_branch_gate,
    wqn, wqr, wld, wkr, cl, cr, wku, wvu, wo, sg, su, dg, du, sd, dd, eg, eu, ed,
    mixed, newlat, newrope,
    tokens, attn_gain, lengths, turns, ids, wts, ffn_gain, latent_gain, branch_gate,
    v_in, v_kr, v_cl, v_cr, v_ku, v_vu, v_wo, v_s, v_d, v_sd, v_dd, v_e, v_ed,
    agx, sendq, recvq, sendo, recvo, senda, recva, sendg, agf, halves,
    sende, recve, ffn_own, ffn_other, sendr, recvr, sendf, recvf,
    kr_pad, by_row, v_it, v_vt, v_ct, w_sem, tp_send, tp_recv, ep_send, ep_recv, pair_send, pair_recv,
):
    T, EP, own, H, nope, rope, latent, cap, scale = sizes
    group = T * own
    R = H * own
    me_t = lax.axis_index("tp")
    me_e = lax.axis_index("ep")
    lat_w = wld.shape[0]

    Z = T // 2
    me_z, me_k = me_t // 2, me_t % 2
    partner = me_t + 1 - 2 * me_k
    width = agx.shape[2]
    half = width // 2
    chips = far_first(me_z, Z)
    order = []
    for z in chips:
        order += [2 * z + me_k, 2 * z + 1 - me_k]
    order.append(partner)

    barrier = pltpu.get_barrier_semaphore()
    for peer in order:
        pl.semaphore_signal(barrier, inc=1, device_id=(me_e, peer), device_id_type=MESH)
    for k in range(1, EP):
        for peer in (me_t, partner):
            pl.semaphore_signal(
                barrier, inc=1, device_id=(flipped(me_e, k, EP), peer), device_id_type=MESH
            )

    n_q, n_r = H * nope, H * rope
    groups = [
        [(h_tokens, tokens)],
        [(h_attn_gain, attn_gain)],
        [
            (wqn, v_in.at[pl.ds(0, n_q)]),
            (wqr, v_in.at[pl.ds(n_q, n_r)]),
            (wld, v_in.at[pl.ds(n_q + n_r, lat_w)]),
        ],
        [(wkr, v_kr)],
        [(wku, v_ku.at[me_k])],
        [(h_lengths, lengths)],
        [(h_turns, turns)],
        [(h_ids, ids)],
        [(h_wts, wts)],
        [(cl, v_cl)],
        [(cr, v_cr)],
        [(wvu, v_vu.at[me_k])],
        [(wo, v_wo.at[me_k])],
        [(h_latent_gain, latent_gain)],
        [(h_ffn_gain, ffn_gain)],
        [(sg, v_s.at[0]), (su, v_s.at[1])],
        [(dg, v_d.at[0]), (du, v_d.at[1])],
        [(sd, v_sd)],
        [(dd, v_dd)],
        [(h_branch_gate, branch_gate)],
        [(eg, v_e.at[0]), (eu, v_e.at[1])],
        [(ed, v_ed)],
    ]
    wholes = {2: v_in, 15: v_s, 16: v_d, 20: v_e}
    first_small, first_cl, first_ffn = 2, 9, 15
    loads = []
    for i, bunch in enumerate(groups):
        for source, target in bunch:
            load = pltpu.make_async_copy(source, target, w_sem.at[i])
            load.start()
        if len(bunch) > 1:
            load = pltpu.make_async_copy(wholes[i], wholes[i], w_sem.at[i])
        loads.append(load)

    sends = []

    def remote(source, target, send_sem, recv_sem, e, t):
        return pltpu.make_async_remote_copy(
            src_ref=source,
            dst_ref=target,
            send_sem=send_sem,
            recv_sem=recv_sem,
            device_id=(e, t),
            device_id_type=MESH,
        )

    def whole(blocks, send_sem, recv_sem):
        every = remote(blocks, blocks, send_sem, recv_sem, me_e, partner)
        sends.append(every)
        return every

    def tp_exchange(phase, source, target):
        sems = tp_send.at[phase], tp_recv.at[phase]
        for peer in order:
            remote(source(peer), target.at[me_t], *sems, me_e, peer).start()
        return whole(target.at[pl.ds(0, T - 1)], *sems)

    def chip_exchange(phase, source, target, core):
        sems = tp_send.at[phase], tp_recv.at[phase]
        for z in chips:
            remote(source(z), target.at[me_z], *sems, me_e, 2 * z + core).start()
        return whole(target.at[pl.ds(0, Z - 1)], *sems)

    def ep_exchange(phase, source, target):
        sems = ep_send.at[phase], ep_recv.at[phase]
        for k in range(EP - 1, 0, -1):
            peer = flipped(me_e, k, EP)
            for c, t in ((me_k, me_t), (1 - me_k, partner)):
                remote(source.at[2 * peer + c], target.at[2 * me_e + me_k], *sems, peer, t).start()
        mine = 2 * me_e + me_k
        remote(source.at[2 * me_e + 1 - me_k], target.at[mine], *sems, me_e, partner).start()
        target[mine] = source[mine]
        return whole(target.at[pl.ds(0, 2 * EP - 1)], *sems)

    def pair_copy(i, source, target):
        copy = remote(source, target, pair_send.at[i], pair_recv.at[i], me_e, partner)
        copy.start()
        sends.append(copy)
        return copy

    def arrive(step):
        step.wait_recv()

    for i in range(first_small):
        loads[i].wait()
    x = tokens[...].astype(F32)
    normed = (x * factor_of(x) * flat(attn_gain[...])).astype(BF16)
    agx[me_z] = normed
    loads[2].wait()
    strip = 4 * lanes

    def turn_weights(i, carry):
        at = pl.ds(pl.multiple_of(i * strip, strip), strip)
        v_it[me_k, at, :] = v_in[:, at].T
        return carry

    lax.fori_loop(0, width // strip, turn_weights, 0)
    pl.semaphore_wait(barrier, T - 1 + 2 * (EP - 1))
    step = chip_exchange(0, lambda z: agx.at[me_z], agx, 1 - me_k)
    for i in range(first_small + 1, first_cl):
        loads[i].wait()
    early = [
        pair_copy(4, v_it.at[me_k], v_it.at[me_k]),
        pair_copy(5, v_ku.at[me_k], v_ku.at[me_k]),
    ]

    slots = EP * 2 * cap
    slot = lax.broadcasted_iota(jnp.int32, (slots, group), 0)
    block = slot // cap
    expert = block // 2 * T + block % 2 + 2 * me_z
    place = (slot - block * cap).astype(F32)
    hit = jnp.zeros((slots, group), F32)
    weight = jnp.zeros((slots, group), F32)
    for k in range(ids.shape[0]):
        same = ids[k : k + 1, :] == expert
        hit = hit + jnp.where(same, 1.0, 0.0)
        weight = weight + jnp.where(same, wts[k : k + 1, :], 0.0)
    upper = jnp.where(
        lax.broadcasted_iota(jnp.int32, (group, group), 0)
        < lax.broadcasted_iota(jnp.int32, (group, group), 1),
        1.0,
        0.0,
    ).astype(BF16)
    rank = nn(hit.astype(BF16), upper)
    dispatch = jnp.where(rank == place, hit, 0.0)
    weight = weight * dispatch
    weight_hi = weight.astype(BF16)
    weight_lo = (weight - weight_hi.astype(F32)).astype(BF16)
    dispatch = dispatch.astype(BF16)

    left = jnp.zeros((own, lanes), jnp.int32)
    row = lax.broadcasted_iota(jnp.int32, (own, lanes), 0)
    for b in range(own):
        left = jnp.where(row == b, lengths[b], left)
    length = left
    bits = turns.shape[0] // 2
    cosine = jnp.ones((own, lanes), F32)
    sine = jnp.zeros((own, lanes), F32)
    for i in range(bits - 1, -1, -1):
        has = left >= 2**i
        left = jnp.where(has, left - 2**i, left)
        c, s = turns[i : i + 1, :], turns[bits + i : bits + i + 1, :]
        cosine, sine = (
            jnp.where(has, cosine * c - sine * s, cosine),
            jnp.where(has, cosine * s + sine * c, sine),
        )
    live = lax.broadcasted_iota(jnp.int32, (own, lanes), 1) < rope
    cosine = jnp.where(live, cosine, 0.0)
    sine = jnp.where(live, sine, 0.0)
    big = T * H
    seq = lax.broadcasted_iota(jnp.int32, (own * big, lanes), 0) // big
    mine = [seq == b for b in range(own)]
    length = spread(length, big)
    cosines, sines = spread(cosine, big), spread(sine, big)
    kr_pad[...] = jnp.zeros_like(kr_pad)
    kr_pad[:, 0:rope] = nt(normed, v_kr[...])
    new_rope = turn(kr_pad[...], cosine, sine, rope // 2).astype(BF16)
    newrope[...] = new_rope[:, 0:rope]

    for copy in early:
        arrive(copy)
    arrive(step)
    rows = rows_of(agx, Z).astype(BF16)
    count = rows.shape[0]
    of_head = lax.broadcasted_iota(jnp.int32, (count, n_q), 1) // nope
    lane = lax.broadcasted_iota(jnp.int32, (count, lanes), 1)
    q_lat, q_rope = [], []
    projected = [nn(rows, v_it[c]) for c in range(2)]
    for c, proj in enumerate(projected):
        every = join([jnp.where(of_head == h, proj[:, 0:n_q], 0.0) for h in range(H)])
        every = nn(every.astype(BF16), join([v_ku[c, h] for h in range(H)]))
        q_lat += [every[count * h : count * (h + 1)] for h in range(H)]
        tail = proj[:, proj.shape[1] - lanes :]
        lat_part = jnp.where(lane >= lanes - lat_w, tail, 0.0)
        for h in range(H):
            offset = n_q + h * rope - (proj.shape[1] - lanes)
            piece = pltpu.roll(tail, lanes - offset, 1) if offset else tail
            q_rope.append(jnp.where(lane < rope, piece, lat_part))
    for z in range(Z):
        cut = slice(own * z, own * (z + 1))
        sendq[z, :, 0:latent] = join([q[cut] for q in q_lat]).astype(BF16)
        sendq[z, :, latent : latent + lanes] = join([q[cut] for q in q_rope]).astype(BF16)
    step = chip_exchange(1, lambda z: sendq.at[z], recvq, 1 - me_k)
    recvq[me_z] = sendq[me_z]
    for i in range(first_cl, first_ffn):
        loads[i].wait()

    per_step = 256

    def turn_keys(i, carry):
        b = i // (v_cl.shape[1] // per_step)
        at = pl.ds(pl.multiple_of(i % (v_cl.shape[1] // per_step) * per_step, lanes), per_step)
        v_ct[b, :, at] = v_cl[b, at, :].T
        return carry

    lax.fori_loop(0, own * (v_cl.shape[1] // per_step), turn_keys, 0)

    arrive(step)
    shared = [
        pair_copy(0, v_vu.at[me_k], v_vu.at[me_k]),
        pair_copy(1, v_wo.at[me_k], v_wo.at[me_k]),
    ]

    queries = rows_of(recvq, Z)
    per = lanes // lat_w
    lane = lax.broadcasted_iota(jnp.int32, (own, lanes), 1)
    blocks = []
    for j in range(T // per):
        total = None
        for i in range(per):
            top = R * (j * per + i)
            piece = jnp.where(lane >= lanes - lat_w, queries[top : top + own, latent:], 0.0)
            if i < per - 1:
                piece = pltpu.roll(piece, (i + 1) * lat_w, 1)
            total = piece if total is None else total + piece
        blocks.append(total)
    raw = blocks[0] if len(blocks) == 1 else jnp.concatenate(blocks, axis=1)
    new_latent = (raw * factor_of(raw) * flat(latent_gain[...])).astype(BF16)
    newlat[...] = new_latent
    new_lat32, new_rope32 = new_latent.astype(F32), new_rope.astype(F32)
    tiles = by_row.shape[0]
    for i in range(tiles):
        by_row[i] = queries[:, lanes * i : lanes * (i + 1)]
    queries = jnp.concatenate(
        [
            join([by_row[i, pl.ds(b, big, stride=own), :] for b in range(own)])
            for i in range(tiles)
        ],
        axis=1,
    )
    q_rot = turn(
        jnp.where(
            lax.broadcasted_iota(jnp.int32, (own * big, lanes), 1) < rope, queries[:, latent:], 0.0
        ),
        cosines,
        sines,
        rope // 2,
    ).astype(BF16).astype(F32)
    q_lat32 = queries[:, 0:latent]
    new_lat_all = spread(new_lat32, big)
    own_score = (
        jnp.sum(q_lat32 * new_lat_all, axis=-1, keepdims=True)
        + jnp.sum(q_rot * spread(new_rope32, big), axis=-1, keepdims=True)
    ) * scale
    across = None
    q_lat16 = q_lat32.astype(BF16)
    for b in range(own):
        turned = pltpu.roll(q_rot, rope * b, 1) if b else q_rot
        turned = jnp.where(mine[b], turned, 0.0)
        across = turned if across is None else across + turned
    across = across[:, 0 : own * rope].astype(BF16)
    depth = v_cl.shape[1] // 2
    scores = []
    for part in range(2):
        cut = slice(part * depth, (part + 1) * depth)
        part = [nn(q_lat16[big * b : big * (b + 1)], v_ct[b, :, cut]) for b in range(own)]
        scores.append(join(part) + nn(across, v_cr[:, cut]))
    scores = jnp.concatenate(scores, axis=1)
    position = lax.broadcasted_iota(jnp.int32, scores.shape, 1)
    scores = jnp.where(position < length[:, 0:1], scores * scale, -jnp.inf)
    peak = jnp.maximum(jnp.max(scores, axis=-1, keepdims=True), own_score)
    past = jnp.exp(scores - peak)
    own_exp = jnp.exp(own_score - peak)
    weights = jnp.sum(past, axis=-1, keepdims=True) + own_exp
    past = past.astype(BF16)
    mixed_lat = []
    for part in range(2):
        cut = slice(part * latent // 2, (part + 1) * latent // 2)
        mixed_lat.append(
            join([nn(past[big * b : big * (b + 1)], v_cl[b, :, cut]) for b in range(own)])
        )
    mixed_lat = jnp.concatenate(mixed_lat, axis=1)
    mixed_lat = (mixed_lat + own_exp * new_lat_all) / weights
    tiles = latent // lanes
    for i in range(tiles):
        for b in range(own):
            block = mixed_lat[big * b : big * (b + 1), lanes * i : lanes * (i + 1)]
            by_row[i, pl.ds(b, big, stride=own), :] = block
    mixed_lat = jnp.concatenate([by_row[i] for i in range(tiles)], axis=1)
    for z in range(Z):
        sendo[z] = mixed_lat[2 * R * z : 2 * R * (z + 1)].astype(BF16)
    step = chip_exchange(2, lambda z: sendo.at[z], recvo, 1 - me_k)
    recvo[me_z] = sendo[me_z]
    for copy in shared:
        arrive(copy)
    for c in range(2):
        v_vt[c] = v_vu[c].T
    arrive(step)

    back = rows_of(recvo, Z).astype(BF16)
    value = jnp.concatenate([nn(back, v_vt[c]) for c in range(2)], axis=1)
    heads = 2 * H
    vhead = value.shape[1] // heads
    at_head = lax.broadcasted_iota(jnp.int32, value.shape, 0) // own % heads
    of_head = lax.broadcasted_iota(jnp.int32, value.shape, 1) // vhead
    value = jnp.where(at_head == of_head, value, 0.0)
    values = []
    for z in range(Z):
        total = None
        for q in range(heads):
            top = own * (heads * z + q)
            term = value[top : top + own]
            total = term if total is None else total + term
        values.append(total)
    values = join(values).astype(BF16)
    for c in range(2):
        cut = slice(c * half, (c + 1) * half)
        part = nn(values, join([v_wo[0, :, cut], v_wo[1, :, cut]]))
        for z in range(Z):
            senda[z, :, cut] = part[own * z : own * (z + 1)].astype(BF16)
    step = chip_exchange(3, lambda z: senda.at[z], recva, 1 - me_k)
    recva[me_z] = senda[me_z]
    arrive(step)
    after = tokens[...].astype(F32)
    for z in range(Z):
        after = after + recva[z].astype(F32)
    normed = (after * factor_of(after) * flat(ffn_gain[...])).astype(BF16)
    for c in range(2):
        sendg[c] = normed[:, c * half : (c + 1) * half]
    step = tp_exchange(4, lambda peer: sendg.at[peer % 2], agf)
    agf[me_t] = sendg[me_k]
    for i in range(first_ffn, len(loads)):
        loads[i].wait()
    arrive(step)

    rows = rows_of(agf, T).astype(BF16)
    halves[me_k] = rows
    outgoing = nn(dispatch, rows)
    for j in range(2 * EP):
        sende[j] = outgoing[cap * j : cap * (j + 1)].astype(BF16)
    step = ep_exchange(0, sende, recve)
    arrive(pair_copy(2, halves.at[me_k], halves.at[me_k]))
    rows = jnp.concatenate([halves[0], halves[1]], axis=1)
    rows32 = rows.astype(F32)
    act = (silu(nt(rows, v_s[0])) * nt(rows, v_s[1])).astype(BF16)
    ffn = nn(act, v_sd[...])
    gate = jnp.sum(rows32 * flat(branch_gate[...].astype(F32)), axis=-1, keepdims=True)
    gate = 1.0 / (1.0 + jnp.exp(-gate))
    act = (silu(nn(rows, v_d[0])) * nn(rows, v_d[1])).astype(BF16)
    ffn = ffn + gate * nn(act, v_dd[...])

    for c in range(2):
        ffn_own[c] = ffn[:, c * half : (c + 1) * half]
    ffn_copy = pair_copy(3, ffn_own.at[1 - me_k], ffn_other)

    arrive(step)
    routed = jnp.concatenate(
        [join([recve[2 * j + c].astype(F32) for j in range(EP)]) for c in range(2)], axis=1
    ).astype(BF16)
    act = (silu(nn(routed, v_e[0])) * nn(routed, v_e[1])).astype(BF16)
    pieces = sendr.shape[0]
    wide = half // pieces
    steps = []
    for n in range(pieces):
        for c in range(2):
            base = c * half + n * wide
            result = nn(act, v_ed[:, base : base + wide])
            for j in range(EP):
                sendr[n, 2 * j + c] = result[cap * j : cap * (j + 1)].astype(BF16)
        steps.append(ep_exchange(1 + n, sendr.at[n], recvr.at[n]))
    arrive(ffn_copy)
    ffn = ffn_own[me_k] + ffn_other[...]
    last = []
    for n in range(pieces):
        arrive(steps[n])
        returned = rows_of(recvr.at[n], 2 * EP).astype(BF16)
        part = ffn[:, n * wide : (n + 1) * wide]
        part = part + (tn(weight_hi, returned) + tn(weight_lo, returned))
        for u in range(T):
            sendf[n, u] = part[own * u : own * (u + 1)].astype(BF16)
        last.append(tp_exchange(5 + n, lambda peer: sendf.at[n, peer], recvf.at[n]))
        recvf[n, me_t] = sendf[n, me_t]
    for n in range(pieces):
        arrive(last[n])
        for c in range(2):
            base = c * half + n * wide
            part = after[:, base : base + wide]
            for z in range(Z):
                part = part + recvf[n, 2 * z + c].astype(F32)
            mixed[:, base : base + wide] = part.astype(BF16)
    for c in sends:
        c.wait_send()


def hand_over(*refs):
    half = len(refs) // 2
    for source, target in zip(refs[:half], refs[half:]):
        target[...] = source[...]


def local(
    tokens, lengths, cache_latent, cache_rope_key, route_ids, route_weights, attn_gain,
    w_query_nope, w_query_rope, w_latent_down, w_key_rope, latent_gain, w_key_up, w_value_up,
    w_attn_out, ffn_gain, expert_gate, expert_up, expert_down, shared_gate, shared_up,
    shared_down, dense_gate, dense_up, dense_down, branch_gate,
):
    own, width = tokens.shape
    T = lax.axis_size("tp")
    EP = lax.axis_size("ep")
    H, nope = w_query_nope.shape[1:]
    rope = w_query_rope.shape[2]
    latent = cache_latent.shape[2]
    top = route_ids.shape[1]
    assert expert_gate.shape[0] == 1
    cap = max(2, (2 * own * top + EP - 1) // EP)
    R = H * own
    half = rope // 2

    bits = cache_latent.shape[1].bit_length()
    frequencies = (rope_base ** (-np.arange(half) / half)).astype(np.float32).astype(np.float64)
    angles = frequencies[None, :] * 2.0 ** np.arange(bits)[:, None]
    angles = np.pad(np.tile(angles, (1, 2)), ((0, 0), (0, lanes - rope)))
    turns = jnp.asarray(np.concatenate([np.cos(angles), np.sin(angles)]), F32)

    operands = (
        tokens,
        attn_gain.reshape(-1, lanes),
        lengths,
        turns,
        route_ids.T,
        route_weights.T,
        ffn_gain.reshape(-1, lanes),
        latent_gain.reshape(-1, lanes),
        branch_gate.reshape(-1, lanes),
        w_query_nope.transpose(1, 2, 0).reshape(H * nope, width),
        w_query_rope.transpose(1, 2, 0).reshape(H * rope, width),
        w_latent_down.T,
        w_key_rope.T,
        cache_latent,
        cache_rope_key.transpose(0, 2, 1).reshape(own * rope, -1),
        w_key_up.transpose(1, 2, 0),
        w_value_up.transpose(1, 2, 0).reshape(-1, latent),
        w_attn_out.reshape(-1, width),
        shared_gate.T,
        shared_up.T,
        dense_gate,
        dense_up,
        shared_down,
        dense_down,
        expert_gate[0],
        expert_up[0],
        expert_down[0],
    )
    big = operands[9:]
    v_in = pltpu.VMEM((sum(o.shape[0] for o in big[:3]), width), BF16)
    pair = (2,)
    weights = [v_in] + [
        pltpu.VMEM(shape, BF16)
        for shape in [o.shape for o in big[3:6]]
        + [pair + o.shape for o in (big[6], big[7], big[8], big[9], big[11])]
        + [big[13].shape, big[14].shape, pair + big[15].shape, big[17].shape]
    ]
    small = [
        (pltpu.SMEM if o is lengths else pltpu.VMEM)(o.shape, o.dtype) for o in operands[:9]
    ]
    q_width = latent + lanes

    def comm(*shape):
        return pltpu.VMEM(shape, BF16)

    half, chips, group, pieces = width // 2, T // 2, T * own, 2
    buffers = [
        comm(chips, own, width),
        comm(chips, 2 * R, q_width), comm(chips, 2 * R, q_width),
        comm(chips, 2 * R, latent), comm(chips, 2 * R, latent),
        comm(chips, own, width), comm(chips, own, width),
        comm(2, own, half),
        comm(T, own, half),
        comm(2, group, half),
        comm(2 * EP, cap, half), comm(2 * EP, cap, half),
        pltpu.VMEM((2, group, half), F32), pltpu.VMEM((group, half), F32),
        comm(pieces, 2 * EP, cap, half // pieces), comm(pieces, 2 * EP, cap, half // pieces),
        comm(pieces, T, own, half // pieces), comm(pieces, T, own, half // pieces),
        pltpu.VMEM((own, lanes), F32),
        pltpu.VMEM((q_width // lanes, T * R, lanes), F32),
        comm(2, width, v_in.shape[0]),
        comm(2, latent, big[7].shape[0]),
        comm(own, latent, cache_latent.shape[1]),
    ]
    n_loads = 22
    sems = [
        pltpu.SemaphoreType.DMA((n_loads,)),
        pltpu.SemaphoreType.DMA((7,)),
        pltpu.SemaphoreType.DMA((7,)),
        pltpu.SemaphoreType.DMA((3,)),
        pltpu.SemaphoreType.DMA((3,)),
        pltpu.SemaphoreType.DMA((6,)),
        pltpu.SemaphoreType.DMA((6,)),
    ]
    sizes = (T, EP, own, H, nope, rope, latent, cap, (nope + rope) ** (-0.5))
    vmem = pl.BlockSpec(memory_space=pltpu.VMEM)
    shapes = [((own, width), BF16), ((own, latent), BF16), ((own, rope), BF16)]
    results = pl.pallas_call(
        functools.partial(layer, sizes),
        out_shape=tuple(pltpu.VMEM(*shape) for shape in shapes),
        in_specs=[pl.BlockSpec(memory_space=pl.ANY)] * len(operands),
        out_specs=(vmem, vmem, vmem),
        scratch_shapes=small + weights + buffers + sems,
        compiler_params=pltpu.CompilerParams(collective_id=0, has_side_effects=True),
    )(*operands)
    return pl.pallas_call(
        hand_over,
        out_shape=tuple(jax.ShapeDtypeStruct(*shape) for shape in shapes),
        in_specs=[vmem] * 3,
        out_specs=(vmem, vmem, vmem),
    )(*[pltpu.with_memory_space_constraint(r, pltpu.VMEM) for r in results])


def solution(mesh):
    both = ("ep", "tp")
    in_specs = (
        P(both, None),
        P(both),
        P(both, None, None),
        P(both, None, None),
        P("ep", None),
        P("ep", None),
        P(),
        P(None, "tp", None),
        P(None, "tp", None),
        P(None, "tp"),
        P(),
        P(),
        P(None, "tp", None),
        P(None, "tp", None),
        P("tp", None, None),
        P(),
        P(both, None, None),
        P(both, None, None),
        P(both, None, None),
        P(None, "tp"),
        P(None, "tp"),
        P("tp", None),
        P(None, "tp"),
        P(None, "tp"),
        P("tp", None),
        P(),
    )
    out_specs = (P(both, None), P(both, None), P(both, None))
    return jax.shard_map(local, mesh=mesh, in_specs=in_specs, out_specs=out_specs, check_vma=False)
```
